32 devices in a mesh: sp: 8 (over z, y), tp: 4 (over x, core).
Axes of the slice: x: 2, y: 2, z: 4, core: 2. Of those that a mesh axis runs over, the one named last changes fastest.
Arguments:
- conv_input: bfloat16 [4096, 1024], P('sp', 'tp'), may hold values from -6 to 6
- gate_inner: bfloat16 [4096, 1024], P('sp', 'tp'), may hold values from -6 to 6
- gate_outer: bfloat16 [4096, 1024], P('sp', 'tp'), may hold values from -6 to 6
- conv_taps: bfloat16 [3, 1024], P(None, 'tp'), may hold values from -3.5 to 3.5
- doc_ids: int32 [4096], P('sp'), may hold values from 0 to 3, never falling along the last dimension, each value on 1 to 2048 neighbouring positions
- residual_in: bfloat16 [4096, 2048], P(('sp', 'tp')), may hold values from -6 to 6
- out_proj: bfloat16 [1024, 2048], replicated, may hold values from -0.1875 to 0.1875
- norm_gain: float32 [2048], replicated, may hold values from 0.1 to 1.9
- expert_ids: int32 [4096, 2], P(('sp', 'tp')), may hold values from 0 to 31, all different within a row; in each aligned block of 128 rows (0 to 127, 128 to 255, ...) at most 16 rows name the same one
- expert_weights: float32 [4096, 2], P(('sp', 'tp')), may hold values from 0.2 to 1
- gate_proj: bfloat16 [32, 2048, 1024], P(('sp', 'tp')), may hold values from -0.125 to 0.125
- up_proj: bfloat16 [32, 2048, 1024], P(('sp', 'tp')), may hold values from -0.125 to 0.125
- down_proj: bfloat16 [32, 1024, 2048], P(('sp', 'tp')), may hold values from -0.1875 to 0.1875
Outputs:
- layer_out: bfloat16 [4096, 2048], P(('sp', 'tp'))
The draws below stay inside these ranges and needn't reach their ends.
Inputs may be any that keep to these rules, and one draw needn't show every extreme that they name: `doc_ids`: never falls along positions; each document has at most 2048 positions. `expert_ids`: each row names 2 different experts; within the rows of one device, aligned blocks of 128 rows, no expert is named more than 16 times, a bound that some block reaches.
All inputs are finite; a program needn't handle non-finite values.
Results may differ from the reference program's by a relative error of at most 0.009.
Values may be sent and summed in bfloat16 or wider, within the bound.
A program may use at most 64 MiB of HBM per device.

```python
import math
import jax
import jax.numpy as jnp
import numpy as np
from jax import lax

D = 2048
CONV = 1024
FF = 1024
KTAPS = 3
TOPK = 2
TOKENS = 4096
ROWS = 128
EXPERTS = 32
CAP = 16
NDOCS = 4
DOC_MOST = 2048


def steps_of(key, shape, cuts, low, top_value):
    level = 1.0
    for axis_at, shards_of in cuts:
        heights = jax.random.uniform(jax.random.fold_in(jax.random.fold_in(key, 6), axis_at), (shards_of,), jnp.float32, low / len(cuts), top_value / len(cuts))
        level = level * jnp.repeat(jnp.exp(heights), shape[axis_at] // shards_of).reshape((-1,) + (1,) * (len(shape) - 1 - axis_at))
    return level


def length_profile(amount, total, most, skew):
    loads = [(1 << 20) // math.isqrt(standing ** skew) + 1 for standing in range(2, amount + 1)]
    surplus, given = total - most - (amount - 1), [1] * (amount - 1)
    while surplus > 0:
        free = [i for i in range(amount - 1) if given[i] < most]
        pool, left = sum([loads[i] for i in free]), surplus
        for i in free:
            more = min(most - given[i], max(1, left * loads[i] // pool), surplus)
            given[i] = given[i] + more
            surplus = surplus - more
    return np.array([most] + given)


def uneven(stream_key, number_of, total, most, slope):
    if number_of == 2:
        one = jax.random.randint(stream_key, (), max(1, total - most), min(most, total - 1) + 1)
        return jnp.stack([one, total - one])
    lengths = jnp.asarray(length_profile(number_of, total, most, slope), jnp.int32)
    twos = (number_of - 1) // 2
    giver, taker = lengths[1:1 + 2 * twos:2], lengths[2:2 + 2 * twos:2]
    slack = jnp.minimum(giver - 1, most - taker)
    shifted = jax.random.randint(jax.random.fold_in(stream_key, 1), (twos,), 0, 1 << 20) % (slack + 1)
    lengths = lengths.at[1:1 + 2 * twos:2].set(giver - shifted).at[2:2 + 2 * twos:2].set(taker + shifted)
    return lengths[jax.random.permutation(jax.random.fold_in(stream_key, 2), number_of)]


def routed_block(rng, own, number, rows, number_of, top, reach, slope):
    ranking = jax.random.permutation(rng, number_of)
    heavy_load, common = portions_of(number_of, rows * top, reach, slope, True), portions_of(number_of, rows * top, reach, slope, False)
    places = jnp.arange(number_of)

    def named(lengths, offset_by):
        used = int((lengths > 0).sum())
        fixed = max(1, used // 4)
        shifted = fixed + (places - fixed + offset_by * (used - fixed)) % max(1, number_of - fixed)
        return jnp.zeros((number_of,), jnp.int32).at[ranking[jnp.where(places < fixed, places, shifted)]].set(jnp.asarray(lengths, jnp.int32))

    lengths = jnp.where(number % 4 == 0, named(heavy_load, number // 4), named(common, number - number // 4 - 1))
    mixed = jax.random.permutation(jax.random.fold_in(own, 3), number_of)
    source_of, taker = mixed[0:number_of // 2 * 2:2], mixed[1:number_of // 2 * 2:2]
    slack = jnp.minimum(lengths[source_of] - 1, reach - lengths[taker]) // 2
    slack = jnp.where((source_of == ranking[0]) | (taker == ranking[0]) | (lengths[taker] == 0), 0, jnp.maximum(slack, 0))
    shifted = jax.random.randint(jax.random.fold_in(own, 4), (number_of // 2,), 0, 1 << 20) % (slack + 1)
    lengths = lengths.at[source_of].add(-shifted).at[taker].add(shifted)
    members = jnp.searchsorted(jnp.cumsum(lengths), jnp.arange(rows * top), side="right").astype(jnp.int32)
    table = members.reshape(top, rows).T
    table = table[jax.random.permutation(jax.random.fold_in(own, 1), rows)]
    offset_by = jax.random.randint(jax.random.fold_in(own, 2), (rows, 1), 0, top)
    return jnp.take_along_axis(table, (jnp.arange(top)[None, :] + offset_by) % top, axis=1)


def portions_of(amount, total, limit, skew, full):
    portions = [(1 << 20) // math.isqrt(rank ** skew) + 1 for rank in range(1, amount + 1)]
    largest = limit if full else min(limit, max(-(-total // amount), total * portions[0] // sum(portions)))
    least = 1 if total - largest >= amount - 1 else 0
    counts, rest = [largest] + [least] * (amount - 1), total - largest - least * (amount - 1)
    while rest > 0:
        free = [i for i in range(1, amount) if counts[i] < largest] or [i for i in range(1, amount) if counts[i] < limit]
        whole, budget = sum([portions[i] for i in free]), rest
        for i in free:
            extra = min(limit - counts[i], max(1, budget * portions[i] // whole), rest)
            counts[i] = counts[i] + extra
            rest = rest - extra
    return np.array(counts)


def gaussian(rng, dims, scale, reach, pieces=(), kind=jnp.bfloat16):
    result = jax.random.normal(rng, dims, jnp.float32) * scale
    if len(pieces) > 0:
        result = steps_of(rng, dims, pieces, -0.22, 0.18) * result
    return jnp.clip(result, min=-reach, max=reach).astype(kind)


def setup_inputs(seed: int = 0) -> dict:
    splits = jax.random.split(jax.random.key(seed), 14)
    conv_input = gaussian(splits[0], (TOKENS, CONV), 1.0, 6.0, ((0, 8), (1, 4)))
    gate_inner = gaussian(splits[1], (TOKENS, CONV), 1.0, 6.0, ((0, 8), (1, 4)))
    gate_outer = gaussian(splits[2], (TOKENS, CONV), 1.0, 6.0, ((0, 8), (1, 4)))
    conv_taps = gaussian(splits[3], (KTAPS, CONV), KTAPS ** -0.5, 3.5, ((1, 4),))
    doc_ids = jnp.searchsorted(jnp.cumsum(uneven(splits[4], NDOCS, TOKENS, DOC_MOST, 0)), jnp.arange(TOKENS), side="right").astype(jnp.int32)
    residual_in = gaussian(splits[5], (TOKENS, D), 1.0, 6.0, ((0, 32),))
    out_proj = gaussian(splits[6], (CONV, D), CONV ** -0.5, 0.1875)
    norm_gain = jnp.clip(1.0 + 0.18 * jax.random.normal(splits[7], (D,), jnp.float32), 0.1, 1.9)
    expert_ids_keys = jax.random.split(jax.random.fold_in(splits[8], 1), TOKENS // ROWS)
    expert_ids_turns = jax.random.permutation(jax.random.fold_in(splits[8], 3), TOKENS // ROWS)
    expert_ids = jax.vmap(lambda own, number: routed_block(jax.random.fold_in(splits[8], 2), own, number, ROWS, EXPERTS, TOPK, CAP, 1))(expert_ids_keys, expert_ids_turns).reshape((TOKENS, TOPK))
    expert_weights = jnp.clip(0.2 + 0.8 * jax.random.uniform(splits[9], (TOKENS, TOPK), jnp.float32) ** steps_of(splits[9], (TOKENS, TOPK), ((0, 32),), -0.2, 0.2), 0.2, 1.0)
    gate_proj = gaussian(splits[10], (EXPERTS, D, FF), D ** -0.5, 0.125, ((0, 32),))
    up_proj = gaussian(splits[11], (EXPERTS, D, FF), D ** -0.5, 0.125, ((0, 32),))
    down_proj = gaussian(splits[12], (EXPERTS, FF, D), FF ** -0.5, 0.1875, ((0, 32),))
    return {"conv_input": conv_input, "gate_inner": gate_inner, "gate_outer": gate_outer, "conv_taps": conv_taps, "doc_ids": doc_ids, "residual_in": residual_in, "out_proj": out_proj, "norm_gain": norm_gain, "expert_ids": expert_ids, "expert_weights": expert_weights, "gate_proj": gate_proj, "up_proj": up_proj, "down_proj": down_proj}


def expert_rows(arrived, gate_weight, up_weight, down_weight):
    gate_value = jnp.dot(arrived, gate_weight, preferred_element_type=jnp.float32)
    up_value = jnp.dot(arrived, up_weight, preferred_element_type=jnp.float32)
    hidden = (jax.nn.silu(gate_value) * up_value).astype(jnp.bfloat16)
    return jnp.dot(hidden, down_weight, preferred_element_type=jnp.float32).astype(jnp.bfloat16)

def reference(conv_input, gate_inner, gate_outer, conv_taps, doc_ids, residual_in, out_proj, norm_gain, expert_ids, expert_weights, gate_proj, up_proj, down_proj):
    inner_prod = conv_input.astype(jnp.float32) * gate_inner.astype(jnp.float32)
    tap_values = conv_taps.astype(jnp.float32)
    channels = inner_prod.shape[1]
    one_rows = jnp.concatenate([jnp.zeros((1, channels), jnp.float32), inner_prod[:-1]], axis=0)
    two_rows = jnp.concatenate([jnp.zeros((2, channels), jnp.float32), inner_prod[:-2]], axis=0)
    one_docs = jnp.concatenate([jnp.full((1,), -1, jnp.int32), doc_ids[:-1]], axis=0)
    two_docs = jnp.concatenate([jnp.full((2,), -1, jnp.int32), doc_ids[:-2]], axis=0)
    one_back = jnp.where((one_docs == doc_ids)[:, None], one_rows, 0.0)
    two_back = jnp.where((two_docs == doc_ids)[:, None], two_rows, 0.0)
    mixed_rows = tap_values[2] * inner_prod + tap_values[1] * one_back + tap_values[0] * two_back
    conv_out = (gate_outer.astype(jnp.float32) * mixed_rows).astype(jnp.bfloat16)
    mix = jnp.dot(conv_out, out_proj, preferred_element_type=jnp.float32).astype(jnp.bfloat16)
    carried = residual_in.astype(jnp.float32) + mix.astype(jnp.float32)
    normed = (carried * lax.rsqrt(lax.optimization_barrier(jnp.mean(carried * carried, axis=1, keepdims=True)) + 1e-06) * norm_gain).astype(jnp.bfloat16)
    choose = expert_ids.shape[1]
    blocks = TOKENS // ROWS
    block_ids = expert_ids.reshape(blocks, ROWS * choose)
    onehot = (block_ids[:, :, None] == jnp.arange(EXPERTS, dtype=jnp.int32)[None, None, :]).astype(jnp.int32)
    slot_rank = lax.optimization_barrier(jnp.sum((jnp.cumsum(onehot, axis=1) - 1) * onehot, axis=2))
    block_index = jnp.arange(blocks, dtype=jnp.int32)[:, None]
    target = (block_ids * (blocks * CAP) + block_index * CAP + slot_rank).reshape(-1).astype(jnp.int32)
    sources = jnp.repeat(normed, choose, axis=0)
    buffer = jnp.zeros((EXPERTS * blocks * CAP, D), jnp.bfloat16).at[target].set(sources)
    buffer = buffer.reshape(EXPERTS, blocks * CAP, D)

    def serve(operands):
        return expert_rows(operands[0], operands[1], operands[2], operands[3])
    results = lax.map(serve, (buffer, gate_proj, up_proj, down_proj))
    picked = results.reshape(-1, D)[target].reshape(TOKENS, choose, D).astype(jnp.float32)
    combined = carried + lax.optimization_barrier(jnp.sum(expert_weights[:, :, None] * picked, axis=1))
    return combined.astype(jnp.bfloat16)
```

```python
import functools

import jax
import jax.numpy as jnp
from jax import lax
from jax.experimental import pallas as pl
from jax.experimental.pallas import tpu as pltpu
from jax.sharding import PartitionSpec as P

MESH = pl.DeviceIdType.MESH
DEPTH = 4


def layer_kernel(
    sp_count, tp_count, cap, pieces,
    conv_hbm, inner_hbm, outer_hbm, taps_hbm, docs_hbm, residual_hbm, gain_hbm, ids_hbm, scores_hbm,
    gate_hbm, up_hbm, down_hbm, proj_hbm,
    out_ref,
    conv_ref, inner_ref, outer_ref, taps_ref, docs_ref, residual_ref, gain_ref, ids_ref, scores_ref,
    gate_w, up_w, down_w, proj_w,
    padded, padded_docs, tail, tail_in, conv_out, conv_in, carried_ref,
    metas, place, wide, high, low, x_all, slots, arrived, served, back, hidden, sums, held, part_out, part_in,
    load_sem, tail_sem, conv_send, conv_recv, meta_send, meta_recv, x_send, x_recv,
    go_send, go_recv, ret_send, ret_recv, part_send, part_recv,
):
    sp = lax.axis_index("sp")
    tp = lax.axis_index("tp")
    span = sp_count // DEPTH
    group = span * tp_count
    z = lax.div(sp, span)
    y = lax.rem(sp, span)
    mine = y * tp_count + tp
    rows, width = carried_ref.shape
    step = width // pieces
    ff = gate_w.shape[1]
    slot_count = group * cap

    low_half = 1 - lax.div(z, DEPTH // 2)
    top = DEPTH - 1
    inward = z * low_half + (top - z) * (1 - low_half)
    is_end = inward == 0

    def flip(k):
        return k * low_half + (top - k) * (1 - low_half)

    def source(end, middle):
        return flip(end * (1 - inward) + middle * inward)

    order = (source(2, 0), source(3, 2), source(1, 3))
    outer_z, inner_z = flip(inward - 1), flip(inward + 1)

    def peer(i):
        return lax.rem(mine + i, group)

    def where(member):
        return (z * span + lax.div(member, tp_count), lax.rem(member, tp_count))

    def along(level):
        return (level * span + y, tp)

    peers = [peer(group - 1 - i) for i in range(group - 1)]
    homes = [where(other) for other in peers]

    pairs = (
        (conv_hbm, conv_ref), (inner_hbm, inner_ref), (docs_hbm, docs_ref), (taps_hbm, taps_ref), (outer_hbm, outer_ref),
        (ids_hbm, ids_ref), (scores_hbm, scores_ref), (residual_hbm, residual_ref), (gain_hbm, gain_ref),
        (proj_hbm, proj_w), (gate_hbm.at[0], gate_w), (up_hbm.at[0], up_w), (down_hbm.at[0], down_w),
    )
    loads = [
        pltpu.make_async_copy(origin, target, load_sem.at[n]) for n, (origin, target) in enumerate(pairs)
    ]
    for load in loads:
        load.start()

    barrier = pltpu.get_barrier_semaphore()
    for home in homes:
        pl.semaphore_signal(barrier, inc=1, device_id=home, device_id_type=MESH)
    levels = [lax.rem(z + i, DEPTH) for i in range(1, DEPTH)]
    for level in levels:
        pl.semaphore_signal(barrier, inc=1, device_id=along(level), device_id_type=MESH)

    @pl.when(sp < sp_count - 1)
    def _():
        pl.semaphore_signal(barrier, inc=1, device_id=(sp + 1, tp), device_id_type=MESH)

    @pl.when(sp > 0)
    def _():
        pl.semaphore_signal(barrier, inc=1, device_id=(sp - 1, tp), device_id_type=MESH)

    length, channels = conv_ref.shape
    lanes = tail.shape[1] - channels
    edge = tail.shape[0]
    for load in loads[:3]:
        load.wait()
    padded[edge:, :] = conv_ref[...].astype(jnp.float32) * inner_ref[...].astype(jnp.float32)
    docs = docs_ref[...].astype(jnp.float32)
    for j in range(length // lanes):
        at = slice(edge + j * lanes, edge + (j + 1) * lanes)
        padded_docs[at, :] = jnp.broadcast_to(docs[j : j + 1, :], (lanes, lanes)).T
    tail[:, :channels] = padded[length:, :]
    tail[:, channels:] = padded_docs[length:, :]
    for load in loads[3:5]:
        load.wait()
    taps = taps_ref[...].astype(jnp.float32)

    def convolve(b):
        first = edge + b * rows
        docs = padded_docs[first : first + rows, :]
        same_one = padded_docs[first - 1 : first - 1 + rows, :] == docs
        same_two = padded_docs[first - 2 : first - 2 + rows, :] == docs
        for k in range(channels // lanes):
            at = slice(k * lanes, (k + 1) * lanes)
            one_back = jnp.where(same_one, padded[first - 1 : first - 1 + rows, at], 0.0)
            two_back = jnp.where(same_two, padded[first - 2 : first - 2 + rows, at], 0.0)
            here = padded[first : first + rows, at]
            mixed = taps[2:3, at] * here + taps[1:2, at] * one_back + taps[0:1, at] * two_back
            gated = outer_ref[b * rows : (b + 1) * rows, at].astype(jnp.float32) * mixed
            conv_out[b, :, at] = gated.astype(jnp.bfloat16)

    def conv_copy(b, landing):
        return pltpu.make_async_remote_copy(
            src_ref=conv_out.at[b], dst_ref=conv_in.at[landing],
            send_sem=conv_send.at[b], recv_sem=conv_recv.at[landing],
            device_id=(sp, b), device_id_type=MESH,
        )

    def hand_out(b):
        @pl.when(tp != b)
        def _():
            conv_copy(b, tp).start()

        @pl.when(tp == b)
        def _():
            conv_in[b] = conv_out[b]

    for b in range(1, tp_count):
        convolve(b)
    for load in loads[5:7]:
        load.wait()
    metas.at[z][0:2, :] = ids_ref[...].astype(jnp.float32)
    metas.at[z][2:4, :] = scores_ref[...]
    metas.at[z][4:, :] = jnp.zeros((4, rows), jnp.float32)

    behind = lax.div(sp + sp_count - 1, sp_count)
    ahead = lax.div(2 * sp_count - 2 - sp, sp_count)
    pl.semaphore_wait(barrier, group - 1 + DEPTH - 1 + behind + ahead)

    tail_copy = pltpu.make_async_remote_copy(
        src_ref=tail, dst_ref=tail_in, send_sem=tail_sem.at[0], recv_sem=tail_sem.at[1],
        device_id=(lax.rem(sp + 1, sp_count), tp), device_id_type=MESH,
    )

    @pl.when(sp < sp_count - 1)
    def _():
        tail_copy.start()

    for b in range(1, tp_count):
        hand_out(b)

    def meta_copy(i):
        return pltpu.make_async_remote_copy(
            src_ref=metas.at[z], dst_ref=metas.at[z], send_sem=meta_send.at[i], recv_sem=meta_recv.at[z],
            device_id=along(levels[i]), device_id_type=MESH,
        )

    def meta_arrival(i):
        return pltpu.make_async_remote_copy(
            src_ref=metas.at[levels[i]], dst_ref=metas.at[levels[i]],
            send_sem=meta_send.at[i], recv_sem=meta_recv.at[levels[i]],
            device_id=along(levels[i]), device_id_type=MESH,
        )

    for i in range(DEPTH - 1):
        meta_copy(i).start()

    first_expert = (z * group).astype(jnp.float32)
    ids = lax.broadcasted_iota(jnp.int32, (group, rows), 0).astype(jnp.float32) + first_expert
    earlier = lax.broadcasted_iota(jnp.int32, (rows, rows), 0) < lax.broadcasted_iota(jnp.int32, (rows, rows), 1)
    earlier = jnp.where(earlier, 1.0, 0.0).astype(jnp.bfloat16)
    seats = lax.broadcasted_iota(jnp.int32, (cap, rows), 0).astype(jnp.float32)

    def choose(s):
        meta = metas.at[s][...]
        taken = jnp.zeros((group, rows), jnp.float32)
        weight = jnp.zeros((group, rows), jnp.float32)
        for k in range(2):
            hit = meta[k : k + 1, :] == ids
            taken = taken + jnp.where(hit, 1.0, 0.0)
            weight = weight + jnp.where(hit, meta[2 + k : 3 + k, :], 0.0)
        rank = jnp.dot(taken.astype(jnp.bfloat16), earlier, preferred_element_type=jnp.float32)
        rank = jnp.where(taken > 0.5, rank, -1.0)
        for e in range(group):
            at = slice(e * cap, (e + 1) * cap)
            seated = rank[e : e + 1, :] == seats
            place.at[s][at, :] = jnp.where(seated, 1.0, 0.0).astype(jnp.bfloat16)
            wide[at, :] = jnp.where(seated, weight[e : e + 1, :], 0.0)
        total = wide[...].T
        upper = total.astype(jnp.bfloat16)
        high.at[s][...] = upper
        low.at[s][...] = (total - upper.astype(jnp.float32)).astype(jnp.bfloat16)

    choose(z)

    @pl.when(sp == 0)
    def _():
        tail_in[:, :channels] = jnp.zeros((edge, channels), jnp.float32)
        tail_in[:, channels:] = jnp.full((edge, lanes), -1.0, jnp.float32)

    @pl.when(sp > 0)
    def _():
        tail_copy.wait_recv()

    padded[:edge, :] = tail_in[:, :channels]
    padded_docs[:edge, :] = tail_in[:, channels:]
    convolve(0)
    hand_out(0)

    for i in range(DEPTH - 1):
        meta_arrival(i).wait_recv()
        choose(levels[i])

    pair = lax.div(tp, 2) * 2
    odd = tp - pair
    givers = [tp, pair + 1 - odd]
    for q in range(1, tp_count // 2):
        base = lax.rem(pair + 2 * q, tp_count)
        givers += [base + odd, base + 1 - odd]

    for load in loads[7:10]:
        load.wait()
    squares = jnp.zeros((rows, 1), jnp.float32)
    for n, giver in enumerate(givers):
        if n > 0:
            conv_copy(0, giver).wait_recv()
        lines = pl.ds(pl.multiple_of(giver * channels, channels), channels)
        block = conv_in.at[giver][...]
        for c in range(pieces):
            at = slice(c * step, (c + 1) * step)
            mix = jnp.dot(block, proj_w[lines, at], preferred_element_type=jnp.float32)
            if n > 0:
                mix = carried_ref[:, at] + mix
            if n == tp_count - 1:
                mix = residual_ref[:, at].astype(jnp.float32) + mix.astype(jnp.bfloat16).astype(jnp.float32)
                squares = squares + jnp.sum(mix * mix, axis=1, keepdims=True)
            carried_ref[:, at] = mix
    scale = lax.rsqrt(squares / width + 1e-06)

    def x_copy(k, s, c, level):
        return pltpu.make_async_remote_copy(
            src_ref=x_all.at[s, c], dst_ref=x_all.at[s, c], send_sem=x_send.at[k, s, c], recv_sem=x_recv.at[s, c],
            device_id=along(level), device_id_type=MESH,
        )

    def part_copy(s, c, slot, level):
        return pltpu.make_async_remote_copy(
            src_ref=part_out.at[s, c], dst_ref=part_in.at[slot, c],
            send_sem=part_send.at[s, c], recv_sem=part_recv.at[slot, c],
            device_id=along(level), device_id_type=MESH,
        )

    def exchange(origin, target, send, recv, s, c, n):
        return pltpu.make_async_remote_copy(
            src_ref=origin.at[s, c, peers[n]], dst_ref=target.at[s, c, mine],
            send_sem=send.at[s, c], recv_sem=recv.at[s, c],
            device_id=homes[n], device_id_type=MESH,
        )

    def everyone(origin, target, send, recv, s, c):
        return pltpu.make_async_remote_copy(
            src_ref=origin.at[s, c, pl.ds(0, group - 1)], dst_ref=target.at[s, c, pl.ds(0, group - 1)],
            send_sem=send.at[s, c], recv_sem=recv.at[s, c],
            device_id=homes[0], device_id_type=MESH,
        )

    go = (slots, arrived, go_send, go_recv)
    ret = (served, back, ret_send, ret_recv)

    def send_all(way, s, c):
        for n in range(group - 1):
            exchange(*way, s, c, n).start()
        way[1].at[s, c, mine][...] = way[0].at[s, c, mine][...]

    def dispatch(s, c, level=None, own=False):
        if not own:
            x_copy(0, s, c, z).wait_recv()
        if level is not None:
            x_copy(0, s, c, level).start()
        picked = jnp.dot(place.at[s][...], x_all.at[s, c][...], preferred_element_type=jnp.float32)
        slots.at[s, c][...] = picked.astype(jnp.bfloat16).reshape(group, cap, step)
        send_all(go, s, c)

    tile = 256

    def serve(s):
        sums[...] = jnp.zeros(sums.shape, jnp.float32)

        @pl.loop(0, pieces)
        def _(c):
            everyone(*go, s, c).wait_recv()
            block = arrived.at[s, c][...].reshape(slot_count, step)
            lines = pl.ds(pl.multiple_of(c * step, step), step)
            for w, weight in enumerate((gate_w, up_w)):
                for f in range(ff // tile):
                    at = slice(f * tile, (f + 1) * tile)
                    to = slice(w * ff + f * tile, w * ff + (f + 1) * tile)
                    sums[:, to] += jnp.dot(block, weight[lines, at], preferred_element_type=jnp.float32)

        gate_value = sums[:, :ff]
        silu = gate_value * (1.0 / (1.0 + jnp.exp(-gate_value)))
        hidden[...] = (silu * sums[:, ff:]).astype(jnp.bfloat16)

        @pl.loop(0, pieces)
        def _(c):
            for f in range(step // tile):
                at = pl.ds(pl.multiple_of(c * step + f * tile, tile), tile)
                value = jnp.dot(hidden[...], down_w[:, at], preferred_element_type=jnp.float32)
                value = value.astype(jnp.bfloat16).reshape(group, cap, tile)
                served.at[s, c][:, :, f * tile : (f + 1) * tile] = value
            send_all(ret, s, c)

    def weighted(s, c):
        everyone(*ret, s, c).wait_recv()
        got = back.at[s, c][...].reshape(slot_count, step)
        return jnp.dot(high.at[s][...], got, preferred_element_type=jnp.float32) + jnp.dot(
            low.at[s][...], got, preferred_element_type=jnp.float32
        )

    def combine_own(c):
        carried_ref[:, c * step : (c + 1) * step] += weighted(z, c)

    def combine(j, c, slot):
        part_out.at[order[j], c][...] = weighted(order[j], c).astype(jnp.bfloat16)
        part_copy(order[j], c, slot, inner_z).start()

    def hold(j, c):
        held[j, c] = weighted(order[j], c)

    def relay(j, c, slot, level):
        part_copy(order[j], c, order[j], level).wait_recv()
        total = held[j, c] + part_in.at[order[j], c][...].astype(jnp.float32)
        part_out.at[order[j], c][...] = total.astype(jnp.bfloat16)
        part_copy(order[j], c, slot, level).start()

    def finish(c, arrivals):
        total = carried_ref[:, c * step : (c + 1) * step]
        for slot in arrivals:
            part_copy(z, c, slot, inner_z).wait_recv()
            total = total + part_in.at[slot, c][...].astype(jnp.float32)
        out_ref[:, c * step : (c + 1) * step] = total.astype(jnp.bfloat16)

    def slot_from(s, above):
        return s + (DEPTH - s) * above

    x_middle = (inner_z, outer_z, outer_z)
    every = range(pieces)

    for c in every:
        at = slice(c * step, (c + 1) * step)
        x_all.at[z, c][...] = (carried_ref[:, at] * scale * gain_ref[:, at]).astype(jnp.bfloat16)
        x_copy(1, z, c, inner_z).start()
        if c == 0:
            @pl.when(inward > 0)
            def _():
                x_copy(0, z, 0, outer_z).start()
    for c in every:
        dispatch(z, c, own=True)
    for load in loads[10:13]:
        load.wait()
    serve(z)

    @pl.when(is_end)
    def _():
        dispatch(order[0], 0)
        for c in every:
            combine_own(c)
        for c in range(1, pieces):
            dispatch(order[0], c)

    @pl.when(inward > 0)
    def _():
        for c in every:
            dispatch(order[0], c, x_middle[0])
            dispatch(order[1], c, x_middle[1])
        dispatch(order[2], 0, x_middle[2])

    serve(order[0])

    def overlap(j):
        for c in range(pieces - 1):
            dispatch(order[j + 1], c)
        for c in range(pieces - 1):
            combine(j, c, order[j])
        dispatch(order[j + 1], pieces - 1)
        combine(j, pieces - 1, order[j])

    @pl.when(is_end)
    def _():
        overlap(0)

    @pl.when(inward > 0)
    def _():
        dispatch(order[2], 1, x_middle[2])

    serve(order[1])

    @pl.when(is_end)
    def _():
        overlap(1)

    @pl.when(inward > 0)
    def _():
        dispatch(order[2], 2, x_middle[2])
        for c in every:
            combine_own(c)
        for c in every:
            hold(0, c)
        for c in range(3, pieces):
            dispatch(order[2], c, x_middle[2])
        for c in range(1, pieces):
            x_copy(0, z, c, outer_z).start()
        for c in every:
            hold(1, c)

    serve(order[2])

    @pl.when(is_end)
    def _():
        for c in every:
            combine(2, c, slot_from(order[2], 1 - low_half))
        for c in every:
            finish(c, (slot_from(z, low_half),))
        for c in every:
            x_copy(1, z, c, inner_z).wait_send()

    @pl.when(inward > 0)
    def _():
        to_middle = slot_from(order[1], 1 - low_half)
        to_end = slot_from(order[0], low_half)
        for c in range(2):
            relay(1, c, to_middle, inner_z)
        for c in every:
            hold(2, c)
        for c in range(2, pieces):
            relay(1, c, to_middle, inner_z)
        for c in every:
            relay(2, c, order[2], inner_z)
            relay(0, c, to_end, outer_z)
        for c in every:
            finish(c, (z, DEPTH))
        for c in every:
            for k, level in enumerate((outer_z, inner_z)):
                x_copy(k, z, c, level).wait_send()
            for j in range(DEPTH - 1):
                x_copy(0, order[j], c, x_middle[j]).wait_send()

    @pl.when(sp < sp_count - 1)
    def _():
        tail_copy.wait_send()

    for b in range(tp_count):
        @pl.when(tp != b)
        def _():
            conv_copy(b, tp).wait_send()

    for i in range(DEPTH - 1):
        meta_copy(i).wait_send()

    @pl.loop(0, DEPTH)
    def _(s):
        @pl.loop(0, pieces)
        def _(c):
            everyone(*go, s, c).wait_send()
            everyone(*ret, s, c).wait_send()

            @pl.when(s != z)
            def _():
                part_copy(s, c, s, inner_z).wait_send()


def run_layer(front, routing, gate_proj, up_proj, down_proj, out_proj, cap, pieces=4):
    sp_count, tp_count = lax.axis_size("sp"), lax.axis_size("tp")
    length, channels = front[0].shape
    lanes = front[4].shape[1]
    rows, width = front[5].shape
    edge = 8
    ff = gate_proj.shape[2]
    group = sp_count // DEPTH * tp_count
    step = width // pieces
    slot_count = group * cap
    slot_shape = (DEPTH, pieces, group, cap, step)
    f32, bf16 = jnp.float32, jnp.bfloat16
    dma = pltpu.SemaphoreType.DMA
    vmem = pltpu.VMEM
    hbm = pl.BlockSpec(memory_space=pl.ANY)
    arrays = (*front, *routing)
    return pl.pallas_call(
        functools.partial(layer_kernel, sp_count, tp_count, cap, pieces),
        out_shape=jax.ShapeDtypeStruct((rows, width), bf16),
        in_specs=[hbm] * (len(arrays) + 4),
        out_specs=pl.BlockSpec(memory_space=pltpu.VMEM),
        scratch_shapes=[vmem(a.shape, a.dtype) for a in arrays]
        + [
            vmem((width, ff), bf16),
            vmem((width, ff), bf16),
            vmem((ff, width), bf16),
            vmem(out_proj.shape, bf16),
            vmem((edge + length, channels), f32),
            vmem((edge + length, lanes), f32),
            vmem((edge, channels + lanes), f32),
            vmem((edge, channels + lanes), f32),
            vmem((tp_count, rows, channels), bf16),
            vmem((tp_count, rows, channels), bf16),
            vmem((rows, width), f32),
            vmem((DEPTH, 8, rows), f32),
            vmem((DEPTH, slot_count, rows), bf16),
            vmem((slot_count, rows), f32),
            vmem((DEPTH, rows, slot_count), bf16),
            vmem((DEPTH, rows, slot_count), bf16),
            vmem((DEPTH, pieces, rows, step), bf16),
            vmem(slot_shape, bf16),
            vmem(slot_shape, bf16),
            vmem(slot_shape, bf16),
            vmem(slot_shape, bf16),
            vmem((slot_count, ff), bf16),
            vmem((slot_count, 2 * ff), f32),
            vmem((DEPTH - 1, pieces, rows, step), f32),
            vmem((DEPTH, pieces, rows, step), bf16),
            vmem((DEPTH + 1, pieces, rows, step), bf16),
            dma((len(arrays) + 4,)),
            dma((2,)),
            dma((tp_count,)),
            dma((tp_count,)),
            dma((DEPTH - 1,)),
            dma((DEPTH,)),
            dma((2, DEPTH, pieces)),
            dma((DEPTH, pieces)),
            dma((DEPTH, pieces)),
            dma((DEPTH, pieces)),
            dma((DEPTH, pieces)),
            dma((DEPTH, pieces)),
            dma((DEPTH, pieces)),
            dma((DEPTH + 1, pieces)),
        ],
        compiler_params=pltpu.CompilerParams(
            collective_id=0, has_side_effects=True, vmem_limit_bytes=56 * 1024 * 1024
        ),
    )(*arrays, gate_proj, up_proj, down_proj, out_proj)


def from_behind(block, axis, distance):
    devices = range(lax.axis_size(axis))
    route = [(i - distance, i) for i in devices if i - distance in devices]
    return lax.ppermute(block, axis, route)


def expert_rows(arrived, gate_weight, up_weight, down_weight):
    gate_value = jnp.dot(arrived, gate_weight, preferred_element_type=jnp.float32)
    up_value = jnp.dot(arrived, up_weight, preferred_element_type=jnp.float32)
    hidden = (jax.nn.silu(gate_value) * up_value).astype(jnp.bfloat16)
    return jnp.dot(hidden, down_weight, preferred_element_type=jnp.float32).astype(jnp.bfloat16)


def on_device(
    conv_input,
    gate_inner,
    gate_outer,
    conv_taps,
    doc_ids,
    residual_in,
    out_proj,
    norm_gain,
    expert_ids,
    expert_weights,
    gate_proj,
    up_proj,
    down_proj,
):
    sp_count, tp_count = lax.axis_size("sp"), lax.axis_size("tp")
    capacity = 2 * residual_in.shape[0] * expert_ids.shape[1] // (sp_count * tp_count)
    if capacity % 16 == 0 and sp_count % DEPTH == 0 and tp_count % 2 == 0:
        docs = doc_ids.reshape(-1, 128)
        front = (conv_input, gate_inner, gate_outer, conv_taps, docs, residual_in, norm_gain[None, :])
        routing = (expert_ids.T, expert_weights.T)
        return run_layer(front, routing, gate_proj, up_proj, down_proj, out_proj, capacity)
    inner_prod = conv_input.astype(jnp.float32) * gate_inner.astype(jnp.float32)
    earlier, earlier_docs = from_behind((inner_prod[-2:], doc_ids[-2:]), "sp", 1)
    padded = jnp.concatenate([earlier, inner_prod], axis=0)
    padded_docs = jnp.concatenate([earlier_docs, doc_ids], axis=0)
    length = inner_prod.shape[0]
    tap_values = conv_taps.astype(jnp.float32)
    one_back = jnp.where(
        (padded_docs[1 : length + 1] == doc_ids)[:, None], padded[1 : length + 1], 0.0
    )
    two_back = jnp.where((padded_docs[:length] == doc_ids)[:, None], padded[:length], 0.0)
    mixed_rows = tap_values[2] * inner_prod + tap_values[1] * one_back + tap_values[0] * two_back
    conv_out = (gate_outer.astype(jnp.float32) * mixed_rows).astype(jnp.bfloat16)
    row_count = residual_in.shape[0]
    regrouped = lax.all_to_all(conv_out, "tp", split_axis=0, concat_axis=1, tiled=True)
    mix = jnp.dot(regrouped, out_proj, preferred_element_type=jnp.float32).astype(jnp.bfloat16)
    carried = residual_in.astype(jnp.float32) + mix.astype(jnp.float32)
    normed = (
        carried * lax.rsqrt(jnp.mean(carried * carried, axis=1, keepdims=True) + 1e-06) * norm_gain
    ).astype(jnp.bfloat16)
    model_width = normed.shape[1]
    choose = expert_ids.shape[1]
    experts_total = sp_count * tp_count
    flat_ids = expert_ids.reshape(-1)
    onehot = (flat_ids[:, None] == jnp.arange(experts_total, dtype=jnp.int32)[None, :]).astype(
        jnp.int32
    )
    slot_rank = jnp.sum((jnp.cumsum(onehot, axis=0) - 1) * onehot, axis=1)
    target = flat_ids * capacity + slot_rank
    sources = jnp.repeat(normed, choose, axis=0)
    outgoing = (
        jnp.zeros((experts_total * capacity, model_width), jnp.bfloat16).at[target].set(sources)
    )
    gate_weight = gate_proj[0]
    up_weight = up_proj[0]
    down_weight = down_proj[0]
    arrived = lax.all_to_all(
        outgoing.reshape(experts_total, capacity, model_width),
        ("sp", "tp"),
        split_axis=0,
        concat_axis=0,
        tiled=True,
    )
    item_count = arrived.shape[1]
    flat_rows = arrived.reshape(-1, model_width)
    result = expert_rows(flat_rows, gate_weight, up_weight, down_weight)
    result = result.reshape(experts_total, item_count, model_width)
    returned = lax.all_to_all(result, ("sp", "tp"), split_axis=0, concat_axis=0, tiled=True)
    picked = (
        returned.reshape(-1, model_width)[target]
        .reshape(row_count, choose, model_width)
        .astype(jnp.float32)
    )
    combined = carried + jnp.sum(expert_weights[:, :, None] * picked, axis=1)
    return combined.astype(jnp.bfloat16)


def solution(mesh):
    in_specs = (
        P("sp", "tp"),
        P("sp", "tp"),
        P("sp", "tp"),
        P(None, "tp"),
        P("sp"),
        P(("sp", "tp"), None),
        P(),
        P(),
        P(("sp", "tp"), None),
        P(("sp", "tp"), None),
        P(("sp", "tp"), None, None),
        P(("sp", "tp"), None, None),
        P(("sp", "tp"), None, None),
    )
    out_specs = P(("sp", "tp"), None)
    return jax.shard_map(
        on_device, mesh=mesh, in_specs=in_specs, out_specs=out_specs, check_vma=False
    )
```

```python
import functools

import jax
import jax.numpy as jnp
from jax import lax
from jax.experimental import pallas as pl
from jax.experimental.pallas import tpu as pltpu
from jax.sharding import PartitionSpec as P

MESH = pl.DeviceIdType.MESH
DEPTH = 4


def layer_kernel(
    sp_count, tp_count, cap, pieces,
    conv_hbm, inner_hbm, outer_hbm, taps_hbm, docs_hbm, residual_hbm, gain_hbm, ids_hbm, scores_hbm,
    gate_hbm, up_hbm, down_hbm, proj_hbm,
    out_ref,
    conv_ref, inner_ref, outer_ref, taps_ref, docs_ref, residual_ref, gain_ref, ids_ref, scores_ref,
    gate_w, up_w, down_w, proj_w,
    padded, padded_docs, tail, tail_in, fix, fix_in, conv_out, conv_in, carried_ref,
    metas, place, wide, high, low, x_all, slots, arrived, served, back, hidden, sums, held, part_out, part_in,
    load_sem, tail_send, tail_recv, fix_send, fix_recv, conv_send, conv_recv, meta_send, meta_recv, x_send, x_recv,
    go_send, go_recv, ret_send, ret_recv, part_send, part_recv,
):
    sp = lax.axis_index("sp")
    tp = lax.axis_index("tp")
    span = sp_count // DEPTH
    group = span * tp_count
    z = lax.div(sp, span)
    y = lax.rem(sp, span)
    mine = y * tp_count + tp
    rows, width = carried_ref.shape
    step = width // pieces
    ff = gate_w.shape[1]
    slot_count = group * cap

    low_half = 1 - lax.div(z, DEPTH // 2)
    top = DEPTH - 1
    inward = z * low_half + (top - z) * (1 - low_half)
    is_end = inward == 0

    def flip(k):
        return k * low_half + (top - k) * (1 - low_half)

    def source(end, middle):
        return flip(end * (1 - inward) + middle * inward)

    order = (source(2, 2), source(3, 0), source(1, 3))
    outer_z, inner_z = flip(inward - 1), flip(inward + 1)

    def where(member):
        return (z * span + lax.div(member, tp_count), lax.rem(member, tp_count))

    def along(level):
        return (level * span + y, tp)

    pair = lax.div(tp, 2) * 2
    odd = tp - pair
    givers = [tp, pair + 1 - odd]
    for q in range(1, tp_count // 2):
        base = lax.rem(pair + 2 * q, tp_count)
        givers += [base + odd, base + 1 - odd]

    peers = []
    for i in range(span - 1, 0, -1):
        side = lax.rem(y + i, span) * tp_count
        peers += [side + t for t in givers[2:]]
    near = [lax.rem(y + i, span) * tp_count + t for i in range(1, span) for t in givers[:2]]
    here = [y * tp_count + t for t in givers[2:]]
    for i in range(max(len(near), len(here))):
        peers += near[i : i + 1] + here[i : i + 1]
    peers.append(y * tp_count + givers[1])
    homes = [where(other) for other in peers]

    pairs = (
        (conv_hbm, conv_ref), (inner_hbm, inner_ref), (docs_hbm, docs_ref), (taps_hbm, taps_ref), (outer_hbm, outer_ref),
        (ids_hbm, ids_ref), (scores_hbm, scores_ref), (residual_hbm, residual_ref), (gain_hbm, gain_ref),
        (proj_hbm, proj_w), (gate_hbm.at[0], gate_w), (up_hbm.at[0], up_w), (down_hbm.at[0], down_w),
    )
    loads = [
        pltpu.make_async_copy(origin, target, load_sem.at[n]) for n, (origin, target) in enumerate(pairs)
    ]
    for load in loads:
        load.start()

    barrier = pltpu.get_barrier_semaphore()
    for home in homes:
        pl.semaphore_signal(barrier, inc=1, device_id=home, device_id_type=MESH)
    levels = [lax.rem(z + i, DEPTH) for i in range(1, DEPTH)]
    for level in levels:
        pl.semaphore_signal(barrier, inc=1, device_id=along(level), device_id_type=MESH)

    for t in range(tp_count):
        @pl.when((tp == 0) & (sp > 0))
        def _():
            pl.semaphore_signal(barrier, inc=1, device_id=(sp - 1, t), device_id_type=MESH)

    length, channels = conv_ref.shape
    lanes = tail.shape[1] - channels
    edge = tail.shape[0]
    for load in loads[:3]:
        load.wait()
    padded[edge:, :] = conv_ref[...].astype(jnp.float32) * inner_ref[...].astype(jnp.float32)
    docs = docs_ref[...].astype(jnp.float32)
    for j in range(length // lanes):
        at = slice(edge + j * lanes, edge + (j + 1) * lanes)
        padded_docs[at, :] = jnp.broadcast_to(docs[j : j + 1, :], (lanes, lanes)).T
    padded[:edge, :] = jnp.zeros((edge, channels), jnp.float32)
    padded_docs[:edge, :] = jnp.full((edge, lanes), -1.0, jnp.float32)
    tail[:, :channels] = padded[length:, :]
    tail[:, channels:] = padded_docs[length:, :]
    for load in loads[3:5]:
        load.wait()
    taps = taps_ref[...].astype(jnp.float32)

    def convolve(b):
        first = edge + b * rows
        docs = padded_docs[first : first + rows, :]
        same_one = padded_docs[first - 1 : first - 1 + rows, :] == docs
        same_two = padded_docs[first - 2 : first - 2 + rows, :] == docs
        for k in range(channels // lanes):
            at = slice(k * lanes, (k + 1) * lanes)
            one_back = jnp.where(same_one, padded[first - 1 : first - 1 + rows, at], 0.0)
            two_back = jnp.where(same_two, padded[first - 2 : first - 2 + rows, at], 0.0)
            here = padded[first : first + rows, at]
            mixed = taps[2:3, at] * here + taps[1:2, at] * one_back + taps[0:1, at] * two_back
            gated = outer_ref[b * rows : (b + 1) * rows, at].astype(jnp.float32) * mixed
            conv_out[b, :, at] = gated.astype(jnp.bfloat16)

    def conv_copy(b, landing):
        return pltpu.make_async_remote_copy(
            src_ref=conv_out.at[b], dst_ref=conv_in.at[landing],
            send_sem=conv_send.at[b], recv_sem=conv_recv.at[landing],
            device_id=(sp, b), device_id_type=MESH,
        )

    def hand_out(b):
        @pl.when(tp != b)
        def _():
            conv_copy(b, tp).start()

        @pl.when(tp == b)
        def _():
            conv_in[b] = conv_out[b]

    for k in range(channels // lanes):
        at = slice(k * lanes, (k + 1) * lanes)
        same_one = padded_docs[edge - 1 : 2 * edge - 1, :] == padded_docs[edge : 2 * edge, :]
        one_back = jnp.where(same_one, padded[edge - 1 : 2 * edge - 1, at], 0.0)
        mixed = taps[2:3, at] * padded[edge : 2 * edge, at] + taps[1:2, at] * one_back
        fix[0:2, at] = mixed[0:2]
    fix[2:4, :] = outer_ref[0:2, :].astype(jnp.float32)
    fix[4:6, :] = taps[0:2]
    fix[6:8, :] = jnp.zeros((2, channels), jnp.float32)

    for b in range(tp_count):
        convolve(b)
    for load in loads[5:7]:
        load.wait()
    metas.at[z][0:2, :] = ids_ref[...].astype(jnp.float32)
    metas.at[z][2:4, :] = scores_ref[...]
    metas.at[z][4:, :] = jnp.zeros((4, rows), jnp.float32)

    ahead = lax.div(2 * sp_count - 2 - sp, sp_count)
    pl.semaphore_wait(barrier, group - 1 + DEPTH - 1 + ahead)

    def tail_copy(t, level):
        return pltpu.make_async_remote_copy(
            src_ref=tail, dst_ref=tail_in.at[t], send_sem=tail_send.at[0], recv_sem=tail_recv.at[t],
            device_id=(level, 0), device_id_type=MESH,
        )

    def fix_copy(t):
        return pltpu.make_async_remote_copy(
            src_ref=fix, dst_ref=fix_in.at[t], send_sem=fix_send.at[0], recv_sem=fix_recv.at[t],
            device_id=(sp, 0), device_id_type=MESH,
        )

    has_next = sp < sp_count - 1
    completes = (tp == 0) & (sp > 0)
    helps = (tp > 0) & (sp > 0)

    @pl.when(has_next)
    def _():
        tail_copy(tp, lax.rem(sp + 1, sp_count)).start()

    for b in range(1, tp_count):
        hand_out(b)

    @pl.when(helps)
    def _():
        fix_copy(tp).start()

    hand_out(0)

    @pl.when(completes)
    def _():
        fix_in[0] = fix[...]

    def complete(n):
        tail_copy(n, sp).wait_recv()
        if n > 0:
            fix_copy(n).wait_recv()
        line = lax.broadcasted_iota(jnp.int32, (16, lanes), 0)
        first_doc, second_doc = padded_docs[edge : edge + 1, :], padded_docs[edge + 1 : edge + 2, :]
        last_doc = tail_in[n, edge - 1 : edge, channels:]
        far_doc = tail_in[n, edge - 2 : edge - 1, channels:]
        for k in range(channels // lanes):
            at = slice(k * lanes, (k + 1) * lanes)
            last, far = tail_in[n, edge - 1 : edge, at], tail_in[n, edge - 2 : edge - 1, at]
            oldest, older = fix_in[n, 4:5, at], fix_in[n, 5:6, at]
            mixed = fix_in[n, 0:1, at] + older * jnp.where(last_doc == first_doc, last, 0.0)
            mixed = mixed + oldest * jnp.where(far_doc == first_doc, far, 0.0)
            row_zero = fix_in[n, 2:3, at] * mixed
            mixed = fix_in[n, 1:2, at] + oldest * jnp.where(last_doc == second_doc, last, 0.0)
            row_one = fix_in[n, 3:4, at] * mixed
            was = conv_in[n, 0:16, at].astype(jnp.float32)
            now = jnp.where(line == 0, row_zero, jnp.where(line == 1, row_one, was))
            conv_in[n, 0:16, at] = now.astype(jnp.bfloat16)


    def meta_copy(i):
        return pltpu.make_async_remote_copy(
            src_ref=metas.at[z], dst_ref=metas.at[z], send_sem=meta_send.at[i], recv_sem=meta_recv.at[z],
            device_id=along(levels[i]), device_id_type=MESH,
        )

    def meta_arrival(i):
        return pltpu.make_async_remote_copy(
            src_ref=metas.at[levels[i]], dst_ref=metas.at[levels[i]],
            send_sem=meta_send.at[i], recv_sem=meta_recv.at[levels[i]],
            device_id=along(levels[i]), device_id_type=MESH,
        )

    for i in range(DEPTH - 1):
        meta_copy(i).start()

    first_expert = (z * group).astype(jnp.float32)
    ids = lax.broadcasted_iota(jnp.int32, (group, rows), 0).astype(jnp.float32) + first_expert
    earlier = lax.broadcasted_iota(jnp.int32, (rows, rows), 0) < lax.broadcasted_iota(jnp.int32, (rows, rows), 1)
    earlier = jnp.where(earlier, 1.0, 0.0).astype(jnp.bfloat16)
    seats = lax.broadcasted_iota(jnp.int32, (cap, rows), 0).astype(jnp.float32)

    def choose(s):
        meta = metas.at[s][...]
        taken = jnp.zeros((group, rows), jnp.float32)
        weight = jnp.zeros((group, rows), jnp.float32)
        for k in range(2):
            hit = meta[k : k + 1, :] == ids
            taken = taken + jnp.where(hit, 1.0, 0.0)
            weight = weight + jnp.where(hit, meta[2 + k : 3 + k, :], 0.0)
        rank = jnp.dot(taken.astype(jnp.bfloat16), earlier, preferred_element_type=jnp.float32)
        rank = jnp.where(taken > 0.5, rank, -1.0)
        for e in range(group):
            at = slice(e * cap, (e + 1) * cap)
            seated = rank[e : e + 1, :] == seats
            place.at[s][at, :] = jnp.where(seated, 1.0, 0.0).astype(jnp.bfloat16)
            wide[at, :] = jnp.where(seated, weight[e : e + 1, :], 0.0)
        total = wide[...].T
        upper = total.astype(jnp.bfloat16)
        high.at[s][...] = upper
        low.at[s][...] = (total - upper.astype(jnp.float32)).astype(jnp.bfloat16)

    choose(z)

    for load in loads[7:10]:
        load.wait()
    squares = jnp.zeros((rows, 1), jnp.float32)
    for n, giver in enumerate(givers):
        if n > 0:
            conv_copy(0, giver).wait_recv()

        @pl.when(completes)
        def _():
            complete(n)

        lines = pl.ds(pl.multiple_of(giver * channels, channels), channels)
        block = conv_in.at[giver][...]
        for c in range(pieces):
            at = slice(c * step, (c + 1) * step)
            mix = jnp.dot(block, proj_w[lines, at], preferred_element_type=jnp.float32)
            if n > 0:
                mix = carried_ref[:, at] + mix
            if n == tp_count - 1:
                mix = residual_ref[:, at].astype(jnp.float32) + mix.astype(jnp.bfloat16).astype(jnp.float32)
                squares = squares + jnp.sum(mix * mix, axis=1, keepdims=True)
            carried_ref[:, at] = mix
    scale = lax.rsqrt(squares / width + 1e-06)

    def x_copy(k, s, c, level):
        return pltpu.make_async_remote_copy(
            src_ref=x_all.at[s, c], dst_ref=x_all.at[s, c], send_sem=x_send.at[k, s, c], recv_sem=x_recv.at[s, c],
            device_id=along(level), device_id_type=MESH,
        )

    def part_copy(s, c, slot, level):
        return pltpu.make_async_remote_copy(
            src_ref=part_out.at[s, c], dst_ref=part_in.at[slot, c],
            send_sem=part_send.at[s, c], recv_sem=part_recv.at[slot, c],
            device_id=along(level), device_id_type=MESH,
        )

    def exchange(origin, target, send, recv, s, c, n):
        return pltpu.make_async_remote_copy(
            src_ref=origin.at[s, c, peers[n]], dst_ref=target.at[s, c, mine],
            send_sem=send.at[s, c], recv_sem=recv.at[s, c],
            device_id=homes[n], device_id_type=MESH,
        )

    def everyone(origin, target, send, recv, s, c):
        return pltpu.make_async_remote_copy(
            src_ref=origin.at[s, c, pl.ds(0, group - 1)], dst_ref=target.at[s, c, pl.ds(0, group - 1)],
            send_sem=send.at[s, c], recv_sem=recv.at[s, c],
            device_id=homes[0], device_id_type=MESH,
        )

    go = (slots, arrived, go_send, go_recv)
    ret = (served, back, ret_send, ret_recv)

    def send_all(way, s, c):
        for n in range(group - 1):
            exchange(*way, s, c, n).start()
        way[1].at[s, c, mine][...] = way[0].at[s, c, mine][...]

    def dispatch(s, c, level=None, own=False):
        if not own:
            x_copy(0, s, c, z).wait_recv()
        if level is not None:
            x_copy(0, s, c, level).start()
        picked = jnp.dot(place.at[s][...], x_all.at[s, c][...], preferred_element_type=jnp.float32)
        slots.at[s, c][...] = picked.astype(jnp.bfloat16).reshape(group, cap, step)
        send_all(go, s, c)

    tile = 256

    def serve_up(s, between=None):
        sums[...] = jnp.zeros(sums.shape, jnp.float32)
        for c in every:
            everyone(*go, s, c).wait_recv()
            block = arrived.at[s, c][...].reshape(slot_count, step)
            lines = slice(c * step, (c + 1) * step)
            for w, weight in enumerate((gate_w, up_w)):
                for f in range(ff // tile):
                    at = slice(f * tile, (f + 1) * tile)
                    to = slice(w * ff + f * tile, w * ff + (f + 1) * tile)
                    sums[:, to] += jnp.dot(block, weight[lines, at], preferred_element_type=jnp.float32)
            if between is not None:
                between(c)
        gate_value = sums[:, :ff]
        silu = gate_value * (1.0 / (1.0 + jnp.exp(-gate_value)))
        hidden[...] = (silu * sums[:, ff:]).astype(jnp.bfloat16)

    def serve_down(s, sends=None):
        @pl.loop(0, pieces)
        def _(c):
            for f in range(step // tile):
                at = pl.ds(pl.multiple_of(c * step + f * tile, tile), tile)
                value = jnp.dot(hidden[...], down_w[:, at], preferred_element_type=jnp.float32)
                value = value.astype(jnp.bfloat16).reshape(group, cap, tile)
                served.at[s, c][:, :, f * tile : (f + 1) * tile] = value
            if sends is True:
                send_all(ret, s, c)
            elif sends is not None:
                pl.when(sends)(lambda: send_all(ret, s, c))

    def weighted(s, c):
        everyone(*ret, s, c).wait_recv()
        got = back.at[s, c][...].reshape(slot_count, step)
        return jnp.dot(high.at[s][...], got, preferred_element_type=jnp.float32) + jnp.dot(
            low.at[s][...], got, preferred_element_type=jnp.float32
        )

    def combine_own(c):
        carried_ref[:, c * step : (c + 1) * step] += weighted(z, c)

    def combine(j, c, slot):
        part_out.at[order[j], c][...] = weighted(order[j], c).astype(jnp.bfloat16)
        part_copy(order[j], c, slot, inner_z).start()

    def hold(j, c):
        held[j, c] = weighted(order[j], c)

    def relay(j, c, slot, level):
        part_copy(order[j], c, order[j], level).wait_recv()
        total = held[j, c] + part_in.at[order[j], c][...].astype(jnp.float32)
        part_out.at[order[j], c][...] = total.astype(jnp.bfloat16)
        part_copy(order[j], c, slot, level).start()

    def finish(c, arrivals):
        total = carried_ref[:, c * step : (c + 1) * step]
        for slot in arrivals:
            part_copy(z, c, slot, inner_z).wait_recv()
            total = total + part_in.at[slot, c][...].astype(jnp.float32)
        out_ref[:, c * step : (c + 1) * step] = total.astype(jnp.bfloat16)

    def slot_from(s, above):
        return s + (DEPTH - s) * above

    x_middle = (outer_z, inner_z, outer_z)
    lead = pieces // 2
    every = range(pieces)

    for c in every:
        at = slice(c * step, (c + 1) * step)
        x_all.at[z, c][...] = (carried_ref[:, at] * scale * gain_ref[:, at]).astype(jnp.bfloat16)
        x_copy(1, z, c, inner_z).start()
        if c < lead:
            @pl.when(inward > 0)
            def _():
                x_copy(0, z, c, outer_z).start()
    for c in every:
        dispatch(z, c, own=True)
    for i in range(DEPTH - 1):
        meta_arrival(i).wait_recv()
        choose(levels[i])
    for load in loads[10:13]:
        load.wait()

    def at_end(todo):
        pl.when(is_end)(todo)

    def in_middle(todo):
        pl.when(inward > 0)(todo)

    def first_hook(c):
        if c == 1:
            @in_middle
            def _():
                dispatch(order[0], 0, x_middle[0])
                dispatch(order[1], 0, x_middle[1])
        if c == 2:
            @at_end
            def _():
                dispatch(order[2], 0)

    serve_up(z, first_hook)

    @in_middle
    def _():
        dispatch(order[0], 1, x_middle[0])
        dispatch(order[1], 1, x_middle[1])

    @at_end
    def _():
        for c in range(1, lead):
            dispatch(order[2], c)

    serve_down(z)

    @at_end
    def _():
        send_all(ret, z, 0)
        send_all(ret, z, 1)
        for c in every:
            dispatch(order[0], c)
            if c + 2 < pieces:
                send_all(ret, z, c + 2)

    @in_middle
    def _():
        for c in range(2, pieces):
            dispatch(order[0], c, x_middle[0])
            dispatch(order[1], c, x_middle[1])

    def second_hook(c):
        if c == 2:
            @in_middle
            def _():
                dispatch(order[2], 0, x_middle[2])

    serve_up(order[0], second_hook)

    @at_end
    def _():
        dispatch(order[1], 0)

    serve_down(order[0], True)

    @at_end
    def _():
        dispatch(order[1], 1)
        for c in every:
            combine_own(c)
        combine(0, 0, order[0])
        dispatch(order[1], 2)
        combine(0, 1, order[0])
        combine(0, 2, order[0])
        dispatch(order[1], 3)
        combine(0, 3, order[0])

    @in_middle
    def _():
        dispatch(order[2], 1, x_middle[2])

    serve_up(order[1])

    @at_end
    def _():
        dispatch(order[2], 2)

    serve_down(order[1], is_end)

    @at_end
    def _():
        dispatch(order[2], 3)
        for c in every:
            combine(1, c, order[1])

    @in_middle
    def _():
        for c in range(2, pieces):
            dispatch(order[2], c, x_middle[2])
        for c in range(lead, pieces):
            x_copy(0, z, c, outer_z).start()
        for c in every:
            send_all(ret, order[1], c)
        for c in every:
            hold(0, c)

    serve_up(order[2])
    serve_down(order[2], True)

    @at_end
    def _():
        for c in every:
            combine(2, c, slot_from(order[2], 1 - low_half))
        for c in every:
            finish(c, (slot_from(z, low_half),))
        for c in every:
            x_copy(1, z, c, inner_z).wait_send()

    @in_middle
    def _():
        to_middle = slot_from(order[0], 1 - low_half)
        to_end = slot_from(order[1], low_half)
        for c in every:
            send_all(ret, z, c)
        relay(0, 0, to_middle, inner_z)
        for c in every:
            hold(1, c)
        relay(0, 1, to_middle, inner_z)
        relay(0, 2, to_middle, inner_z)
        hold(2, 0)
        hold(2, 1)
        relay(0, 3, to_middle, inner_z)
        hold(2, 2)
        hold(2, 3)
        relay(2, 0, order[2], inner_z)
        for c in every:
            combine_own(c)
        for c in range(1, pieces + 1):
            if c < pieces:
                relay(2, c, order[2], inner_z)
            relay(1, c - 1, to_end, outer_z)
        for c in every:
            finish(c, (z, DEPTH))
        for c in every:
            for k, level in enumerate((outer_z, inner_z)):
                x_copy(k, z, c, level).wait_send()
            for j in range(DEPTH - 1):
                x_copy(0, order[j], c, x_middle[j]).wait_send()

    @pl.when(has_next)
    def _():
        tail_copy(tp, lax.rem(sp + 1, sp_count)).wait_send()

    @pl.when(helps)
    def _():
        fix_copy(tp).wait_send()

    for b in range(tp_count):
        @pl.when(tp != b)
        def _():
            conv_copy(b, tp).wait_send()

    for i in range(DEPTH - 1):
        meta_copy(i).wait_send()

    @pl.loop(0, DEPTH)
    def _(s):
        @pl.loop(0, pieces)
        def _(c):
            everyone(*go, s, c).wait_send()
            everyone(*ret, s, c).wait_send()

            @pl.when(s != z)
            def _():
                part_copy(s, c, s, inner_z).wait_send()


def run_layer(front, routing, gate_proj, up_proj, down_proj, out_proj, cap, pieces=4):
    sp_count, tp_count = lax.axis_size("sp"), lax.axis_size("tp")
    length, channels = front[0].shape
    lanes = front[4].shape[1]
    rows, width = front[5].shape
    edge = 8
    ff = gate_proj.shape[2]
    group = sp_count // DEPTH * tp_count
    step = width // pieces
    slot_count = group * cap
    slot_shape = (DEPTH, pieces, group, cap, step)
    f32, bf16 = jnp.float32, jnp.bfloat16
    dma = pltpu.SemaphoreType.DMA
    vmem = pltpu.VMEM
    hbm = pl.BlockSpec(memory_space=pl.ANY)
    arrays = (*front, *routing)
    return pl.pallas_call(
        functools.partial(layer_kernel, sp_count, tp_count, cap, pieces),
        out_shape=jax.ShapeDtypeStruct((rows, width), bf16),
        in_specs=[hbm] * (len(arrays) + 4),
        out_specs=pl.BlockSpec(memory_space=pltpu.VMEM),
        scratch_shapes=[vmem(a.shape, a.dtype) for a in arrays]
        + [
            vmem((width, ff), bf16),
            vmem((width, ff), bf16),
            vmem((ff, width), bf16),
            vmem(out_proj.shape, bf16),
            vmem((edge + length, channels), f32),
            vmem((edge + length, lanes), f32),
            vmem((edge, channels + lanes), f32),
            vmem((tp_count, edge, channels + lanes), f32),
            vmem((edge, channels), f32),
            vmem((tp_count, edge, channels), f32),
            vmem((tp_count, rows, channels), bf16),
            vmem((tp_count, rows, channels), bf16),
            vmem((rows, width), f32),
            vmem((DEPTH, 8, rows), f32),
            vmem((DEPTH, slot_count, rows), bf16),
            vmem((slot_count, rows), f32),
            vmem((DEPTH, rows, slot_count), bf16),
            vmem((DEPTH, rows, slot_count), bf16),
            vmem((DEPTH, pieces, rows, step), bf16),
            vmem(slot_shape, bf16),
            vmem(slot_shape, bf16),
            vmem(slot_shape, bf16),
            vmem(slot_shape, bf16),
            vmem((slot_count, ff), bf16),
            vmem((slot_count, 2 * ff), f32),
            vmem((DEPTH - 1, pieces, rows, step), f32),
            vmem((DEPTH, pieces, rows, step), bf16),
            vmem((DEPTH + 1, pieces, rows, step), bf16),
            dma((len(arrays) + 4,)),
            dma((1,)),
            dma((tp_count,)),
            dma((1,)),
            dma((tp_count,)),
            dma((tp_count,)),
            dma((tp_count,)),
            dma((DEPTH - 1,)),
            dma((DEPTH,)),
            dma((2, DEPTH, pieces)),
            dma((DEPTH, pieces)),
            dma((DEPTH, pieces)),
            dma((DEPTH, pieces)),
            dma((DEPTH, pieces)),
            dma((DEPTH, pieces)),
            dma((DEPTH, pieces)),
            dma((DEPTH + 1, pieces)),
        ],
        compiler_params=pltpu.CompilerParams(
            collective_id=0, has_side_effects=True, vmem_limit_bytes=56 * 1024 * 1024
        ),
    )(*arrays, gate_proj, up_proj, down_proj, out_proj)


def from_behind(block, axis, distance):
    devices = range(lax.axis_size(axis))
    route = [(i - distance, i) for i in devices if i - distance in devices]
    return lax.ppermute(block, axis, route)


def expert_rows(arrived, gate_weight, up_weight, down_weight):
    gate_value = jnp.dot(arrived, gate_weight, preferred_element_type=jnp.float32)
    up_value = jnp.dot(arrived, up_weight, preferred_element_type=jnp.float32)
    hidden = (jax.nn.silu(gate_value) * up_value).astype(jnp.bfloat16)
    return jnp.dot(hidden, down_weight, preferred_element_type=jnp.float32).astype(jnp.bfloat16)


def on_device(
    conv_input,
    gate_inner,
    gate_outer,
    conv_taps,
    doc_ids,
    residual_in,
    out_proj,
    norm_gain,
    expert_ids,
    expert_weights,
    gate_proj,
    up_proj,
    down_proj,
):
    sp_count, tp_count = lax.axis_size("sp"), lax.axis_size("tp")
    capacity = 2 * residual_in.shape[0] * expert_ids.shape[1] // (sp_count * tp_count)
    if capacity % 16 == 0 and sp_count % DEPTH == 0 and tp_count % 2 == 0:
        docs = doc_ids.reshape(-1, 128)
        front = (conv_input, gate_inner, gate_outer, conv_taps, docs, residual_in, norm_gain[None, :])
        routing = (expert_ids.T, expert_weights.T)
        return run_layer(front, routing, gate_proj, up_proj, down_proj, out_proj, capacity)
    inner_prod = conv_input.astype(jnp.float32) * gate_inner.astype(jnp.float32)
    earlier, earlier_docs = from_behind((inner_prod[-2:], doc_ids[-2:]), "sp", 1)
    padded = jnp.concatenate([earlier, inner_prod], axis=0)
    padded_docs = jnp.concatenate([earlier_docs, doc_ids], axis=0)
    length = inner_prod.shape[0]
    tap_values = conv_taps.astype(jnp.float32)
    one_back = jnp.where(
        (padded_docs[1 : length + 1] == doc_ids)[:, None], padded[1 : length + 1], 0.0
    )
    two_back = jnp.where((padded_docs[:length] == doc_ids)[:, None], padded[:length], 0.0)
    mixed_rows = tap_values[2] * inner_prod + tap_values[1] * one_back + tap_values[0] * two_back
    conv_out = (gate_outer.astype(jnp.float32) * mixed_rows).astype(jnp.bfloat16)
    row_count = residual_in.shape[0]
    regrouped = lax.all_to_all(conv_out, "tp", split_axis=0, concat_axis=1, tiled=True)
    mix = jnp.dot(regrouped, out_proj, preferred_element_type=jnp.float32).astype(jnp.bfloat16)
    carried = residual_in.astype(jnp.float32) + mix.astype(jnp.float32)
    normed = (
        carried * lax.rsqrt(jnp.mean(carried * carried, axis=1, keepdims=True) + 1e-06) * norm_gain
    ).astype(jnp.bfloat16)
    model_width = normed.shape[1]
    choose = expert_ids.shape[1]
    experts_total = sp_count * tp_count
    flat_ids = expert_ids.reshape(-1)
    onehot = (flat_ids[:, None] == jnp.arange(experts_total, dtype=jnp.int32)[None, :]).astype(
        jnp.int32
    )
    slot_rank = jnp.sum((jnp.cumsum(onehot, axis=0) - 1) * onehot, axis=1)
    target = flat_ids * capacity + slot_rank
    sources = jnp.repeat(normed, choose, axis=0)
    outgoing = (
        jnp.zeros((experts_total * capacity, model_width), jnp.bfloat16).at[target].set(sources)
    )
    gate_weight = gate_proj[0]
    up_weight = up_proj[0]
    down_weight = down_proj[0]
    arrived = lax.all_to_all(
        outgoing.reshape(experts_total, capacity, model_width),
        ("sp", "tp"),
        split_axis=0,
        concat_axis=0,
        tiled=True,
    )
    item_count = arrived.shape[1]
    flat_rows = arrived.reshape(-1, model_width)
    result = expert_rows(flat_rows, gate_weight, up_weight, down_weight)
    result = result.reshape(experts_total, item_count, model_width)
    returned = lax.all_to_all(result, ("sp", "tp"), split_axis=0, concat_axis=0, tiled=True)
    picked = (
        returned.reshape(-1, model_width)[target]
        .reshape(row_count, choose, model_width)
        .astype(jnp.float32)
    )
    combined = carried + jnp.sum(expert_weights[:, :, None] * picked, axis=1)
    return combined.astype(jnp.bfloat16)


def solution(mesh):
    in_specs = (
        P("sp", "tp"),
        P("sp", "tp"),
        P("sp", "tp"),
        P(None, "tp"),
        P("sp"),
        P(("sp", "tp"), None),
        P(),
        P(),
        P(("sp", "tp"), None),
        P(("sp", "tp"), None),
        P(("sp", "tp"), None, None),
        P(("sp", "tp"), None, None),
        P(("sp", "tp"), None, None),
    )
    out_specs = P(("sp", "tp"), None)
    return jax.shard_map(
        on_device, mesh=mesh, in_specs=in_specs, out_specs=out_specs, check_vma=False
    )
```

```python
import functools

import jax
import jax.numpy as jnp
from jax import lax
from jax.experimental import pallas as pl
from jax.experimental.pallas import tpu as pltpu
from jax.sharding import PartitionSpec as P

MESH = pl.DeviceIdType.MESH
DEPTH = 4


def layer_kernel(
    sp_count, tp_count, cap, pieces,
    conv_hbm, inner_hbm, outer_hbm, taps_hbm, docs_hbm, residual_hbm, gain_hbm, ids_hbm, scores_hbm,
    gate_hbm, up_hbm, down_hbm, proj_hbm,
    out_ref,
    conv_ref, inner_ref, outer_ref, taps_ref, docs_ref, residual_ref, gain_ref, ids_ref, scores_ref,
    gate_w, up_w, down_w, proj_w,
    padded, padded_docs, tail, tail_in, fix, fix_in, conv_out, conv_in, carried_ref,
    metas, place, wide, high, low, x_all, slots, arrived, served, back, hidden, sums, held, part_out, part_in,
    load_sem, tail_send, tail_recv, fix_send, fix_recv, conv_send, conv_recv, meta_send, meta_recv, x_send, x_recv,
    go_send, go_recv, ret_send, ret_recv, part_send, part_recv,
):
    sp = lax.axis_index("sp")
    tp = lax.axis_index("tp")
    span = sp_count // DEPTH
    group = span * tp_count
    z = lax.div(sp, span)
    y = lax.rem(sp, span)
    mine = y * tp_count + tp
    rows, width = carried_ref.shape
    step = width // pieces
    ff = gate_w.shape[1]
    slot_count = group * cap

    low_half = 1 - lax.div(z, DEPTH // 2)
    top = DEPTH - 1
    inward = z * low_half + (top - z) * (1 - low_half)
    is_end = inward == 0

    def flip(k):
        return k * low_half + (top - k) * (1 - low_half)

    def source(end, middle):
        return flip(end * (1 - inward) + middle * inward)

    order = (source(2, 2), source(3, 0), source(1, 3))
    outer_z, inner_z = flip(inward - 1), flip(inward + 1)

    def where(member):
        return (z * span + lax.div(member, tp_count), lax.rem(member, tp_count))

    def along(level):
        return (level * span + y, tp)

    pair = lax.div(tp, 2) * 2
    odd = tp - pair
    givers = [tp, pair + 1 - odd]
    for q in range(1, tp_count // 2):
        base = lax.rem(pair + 2 * q, tp_count)
        givers += [base + odd, base + 1 - odd]

    peers = []
    for i in range(span - 1, 0, -1):
        side = lax.rem(y + i, span) * tp_count
        peers += [side + t for t in givers[2:]]
    near = [lax.rem(y + i, span) * tp_count + t for i in range(1, span) for t in givers[:2]]
    here = [y * tp_count + t for t in givers[2:]]
    for i in range(max(len(near), len(here))):
        peers += near[i : i + 1] + here[i : i + 1]
    peers.append(y * tp_count + givers[1])
    homes = [where(other) for other in peers]

    pairs = (
        (conv_hbm, conv_ref), (inner_hbm, inner_ref), (docs_hbm, docs_ref), (taps_hbm, taps_ref), (outer_hbm, outer_ref),
        (ids_hbm, ids_ref), (scores_hbm, scores_ref), (residual_hbm, residual_ref), (gain_hbm, gain_ref),
        (proj_hbm, proj_w), (gate_hbm.at[0], gate_w), (up_hbm.at[0], up_w), (down_hbm.at[0], down_w),
    )
    loads = [
        pltpu.make_async_copy(origin, target, load_sem.at[n]) for n, (origin, target) in enumerate(pairs)
    ]
    for load in loads:
        load.start()

    barrier = pltpu.get_barrier_semaphore()
    for home in homes:
        pl.semaphore_signal(barrier, inc=1, device_id=home, device_id_type=MESH)
    pl.semaphore_signal(barrier, inc=1, device_id=along(inner_z), device_id_type=MESH)

    @pl.when(inward > 0)
    def _():
        pl.semaphore_signal(barrier, inc=1, device_id=along(outer_z), device_id_type=MESH)

    for t in range(tp_count):
        @pl.when((tp == 0) & (sp > 0))
        def _():
            pl.semaphore_signal(barrier, inc=1, device_id=(sp - 1, t), device_id_type=MESH)

    length, channels = conv_ref.shape
    lanes = tail.shape[1] - channels
    edge = tail.shape[0]
    for load in loads[:3]:
        load.wait()
    padded[edge:, :] = conv_ref[...].astype(jnp.float32) * inner_ref[...].astype(jnp.float32)
    docs = docs_ref[...].astype(jnp.float32)
    for j in range(length // lanes):
        at = slice(edge + j * lanes, edge + (j + 1) * lanes)
        padded_docs[at, :] = jnp.broadcast_to(docs[j : j + 1, :], (lanes, lanes)).T
    padded[:edge, :] = jnp.zeros((edge, channels), jnp.float32)
    padded_docs[:edge, :] = jnp.full((edge, lanes), -1.0, jnp.float32)
    tail[:, :channels] = padded[length:, :]
    tail[:, channels:] = padded_docs[length:, :]
    for load in loads[3:5]:
        load.wait()
    taps = taps_ref[...].astype(jnp.float32)

    def convolve(b):
        first = edge + b * rows
        docs = padded_docs[first : first + rows, :]
        same_one = padded_docs[first - 1 : first - 1 + rows, :] == docs
        same_two = padded_docs[first - 2 : first - 2 + rows, :] == docs
        for k in range(channels // lanes):
            at = slice(k * lanes, (k + 1) * lanes)
            one_back = jnp.where(same_one, padded[first - 1 : first - 1 + rows, at], 0.0)
            two_back = jnp.where(same_two, padded[first - 2 : first - 2 + rows, at], 0.0)
            here = padded[first : first + rows, at]
            mixed = taps[2:3, at] * here + taps[1:2, at] * one_back + taps[0:1, at] * two_back
            gated = outer_ref[b * rows : (b + 1) * rows, at].astype(jnp.float32) * mixed
            conv_out[b, :, at] = gated.astype(jnp.bfloat16)

    def conv_copy(b, landing):
        return pltpu.make_async_remote_copy(
            src_ref=conv_out.at[b], dst_ref=conv_in.at[landing],
            send_sem=conv_send.at[b], recv_sem=conv_recv.at[landing],
            device_id=(sp, b), device_id_type=MESH,
        )

    def hand_out(b):
        @pl.when(tp != b)
        def _():
            conv_copy(b, tp).start()

        @pl.when(tp == b)
        def _():
            conv_in[b] = conv_out[b]

    for k in range(channels // lanes):
        at = slice(k * lanes, (k + 1) * lanes)
        same_one = padded_docs[edge - 1 : 2 * edge - 1, :] == padded_docs[edge : 2 * edge, :]
        one_back = jnp.where(same_one, padded[edge - 1 : 2 * edge - 1, at], 0.0)
        mixed = taps[2:3, at] * padded[edge : 2 * edge, at] + taps[1:2, at] * one_back
        fix[0:2, at] = mixed[0:2]
    fix[2:4, :] = outer_ref[0:2, :].astype(jnp.float32)
    fix[4:6, :] = taps[0:2]
    fix[6:8, :] = jnp.zeros((2, channels), jnp.float32)

    for b in range(tp_count):
        convolve(b)
    for load in loads[5:7]:
        load.wait()
    metas.at[z][0:2, :] = ids_ref[...].astype(jnp.float32)
    metas.at[z][2:4, :] = scores_ref[...]
    metas.at[z][4:, :] = jnp.zeros((4, rows), jnp.float32)

    ahead = lax.div(2 * sp_count - 2 - sp, sp_count)
    pl.semaphore_wait(barrier, group + inward + ahead)

    def tail_copy(t, level):
        return pltpu.make_async_remote_copy(
            src_ref=tail, dst_ref=tail_in.at[t], send_sem=tail_send.at[0], recv_sem=tail_recv.at[t],
            device_id=(level, 0), device_id_type=MESH,
        )

    def fix_copy(t):
        return pltpu.make_async_remote_copy(
            src_ref=fix, dst_ref=fix_in.at[t], send_sem=fix_send.at[0], recv_sem=fix_recv.at[t],
            device_id=(sp, 0), device_id_type=MESH,
        )

    has_next = sp < sp_count - 1
    completes = (tp == 0) & (sp > 0)
    helps = (tp > 0) & (sp > 0)

    @pl.when(has_next)
    def _():
        tail_copy(tp, lax.rem(sp + 1, sp_count)).start()

    hand_out(0)

    @pl.when(helps)
    def _():
        fix_copy(tp).start()

    for b in range(1, tp_count):
        hand_out(b)

    @pl.when(completes)
    def _():
        fix_in[0] = fix[...]

    def complete(n):
        tail_copy(n, sp).wait_recv()
        if n > 0:
            fix_copy(n).wait_recv()
        line = lax.broadcasted_iota(jnp.int32, (16, lanes), 0)
        first_doc, second_doc = padded_docs[edge : edge + 1, :], padded_docs[edge + 1 : edge + 2, :]
        last_doc = tail_in[n, edge - 1 : edge, channels:]
        far_doc = tail_in[n, edge - 2 : edge - 1, channels:]
        for k in range(channels // lanes):
            at = slice(k * lanes, (k + 1) * lanes)
            last, far = tail_in[n, edge - 1 : edge, at], tail_in[n, edge - 2 : edge - 1, at]
            oldest, older = fix_in[n, 4:5, at], fix_in[n, 5:6, at]
            mixed = fix_in[n, 0:1, at] + older * jnp.where(last_doc == first_doc, last, 0.0)
            mixed = mixed + oldest * jnp.where(far_doc == first_doc, far, 0.0)
            row_zero = fix_in[n, 2:3, at] * mixed
            mixed = fix_in[n, 1:2, at] + oldest * jnp.where(last_doc == second_doc, last, 0.0)
            row_one = fix_in[n, 3:4, at] * mixed
            was = conv_in[n, 0:16, at].astype(jnp.float32)
            now = jnp.where(line == 0, row_zero, jnp.where(line == 1, row_one, was))
            conv_in[n, 0:16, at] = now.astype(jnp.bfloat16)


    def meta_copy(k, s, level):
        return pltpu.make_async_remote_copy(
            src_ref=metas.at[s], dst_ref=metas.at[s], send_sem=meta_send.at[k], recv_sem=meta_recv.at[s],
            device_id=along(level), device_id_type=MESH,
        )

    meta_copy(0, z, inner_z).start()

    @pl.when(inward > 0)
    def _():
        meta_copy(1, z, outer_z).start()

    first_expert = (z * group).astype(jnp.float32)
    ids = lax.broadcasted_iota(jnp.int32, (group, rows), 0).astype(jnp.float32) + first_expert
    earlier = lax.broadcasted_iota(jnp.int32, (rows, rows), 0) < lax.broadcasted_iota(jnp.int32, (rows, rows), 1)
    earlier = jnp.where(earlier, 1.0, 0.0).astype(jnp.bfloat16)
    seats = lax.broadcasted_iota(jnp.int32, (cap, rows), 0).astype(jnp.float32)

    def choose(s):
        meta = metas.at[s][...]
        taken = jnp.zeros((group, rows), jnp.float32)
        weight = jnp.zeros((group, rows), jnp.float32)
        for k in range(2):
            hit = meta[k : k + 1, :] == ids
            taken = taken + jnp.where(hit, 1.0, 0.0)
            weight = weight + jnp.where(hit, meta[2 + k : 3 + k, :], 0.0)
        rank = jnp.dot(taken.astype(jnp.bfloat16), earlier, preferred_element_type=jnp.float32)
        rank = jnp.where(taken > 0.5, rank, -1.0)
        for e in range(group):
            at = slice(e * cap, (e + 1) * cap)
            seated = rank[e : e + 1, :] == seats
            place.at[s][at, :] = jnp.where(seated, 1.0, 0.0).astype(jnp.bfloat16)
            wide[at, :] = jnp.where(seated, weight[e : e + 1, :], 0.0)
        total = wide[...].T
        upper = total.astype(jnp.bfloat16)
        high.at[s][...] = upper
        low.at[s][...] = (total - upper.astype(jnp.float32)).astype(jnp.bfloat16)

    choose(z)

    for load in loads[7:10]:
        load.wait()
    squares = jnp.zeros((rows, 1), jnp.float32)
    for n, giver in enumerate(givers):
        if n > 0:
            conv_copy(0, giver).wait_recv()

        @pl.when(completes)
        def _():
            complete(n)

        lines = pl.ds(pl.multiple_of(giver * channels, channels), channels)
        block = conv_in.at[giver][...]
        for c in range(pieces):
            at = slice(c * step, (c + 1) * step)
            mix = jnp.dot(block, proj_w[lines, at], preferred_element_type=jnp.float32)
            if n > 0:
                mix = carried_ref[:, at] + mix
            if n == tp_count - 1:
                mix = residual_ref[:, at].astype(jnp.float32) + mix.astype(jnp.bfloat16).astype(jnp.float32)
                squares = squares + jnp.sum(mix * mix, axis=1, keepdims=True)
            carried_ref[:, at] = mix
    scale = lax.rsqrt(squares / width + 1e-06)

    def x_copy(k, s, c, level):
        return pltpu.make_async_remote_copy(
            src_ref=x_all.at[s, c], dst_ref=x_all.at[s, c], send_sem=x_send.at[k], recv_sem=x_recv.at[s, c],
            device_id=along(level), device_id_type=MESH,
        )

    def part_copy(s, c, slot, level):
        return pltpu.make_async_remote_copy(
            src_ref=part_out.at[s, c], dst_ref=part_in.at[slot, c],
            send_sem=part_send.at[0], recv_sem=part_recv.at[slot, c],
            device_id=along(level), device_id_type=MESH,
        )

    def exchange(origin, target, send, recv, s, c, n):
        return pltpu.make_async_remote_copy(
            src_ref=origin.at[s, c, peers[n]], dst_ref=target.at[s, c, mine],
            send_sem=send.at[0], recv_sem=recv.at[s, c],
            device_id=homes[n], device_id_type=MESH,
        )

    def everyone(origin, target, send, recv, s, c):
        return pltpu.make_async_remote_copy(
            src_ref=origin.at[s, c, pl.ds(0, group - 1)], dst_ref=target.at[s, c, pl.ds(0, group - 1)],
            send_sem=send.at[0], recv_sem=recv.at[s, c],
            device_id=homes[0], device_id_type=MESH,
        )

    go = (slots, arrived, go_send, go_recv)
    ret = (served, back, ret_send, ret_recv)

    def send_all(way, s, c):
        for n in range(group - 1):
            exchange(*way, s, c, n).start()
        way[1].at[s, c, mine][...] = way[0].at[s, c, mine][...]

    def dispatch(s, c, level=None, own=False):
        if not own:
            x_copy(0, s, c, z).wait_recv()
        if level is not None:
            x_copy(0, s, c, level).start()
        picked = jnp.dot(place.at[s][...], x_all.at[s, c][...], preferred_element_type=jnp.float32)
        slots.at[s, c][...] = picked.astype(jnp.bfloat16).reshape(group, cap, step)
        send_all(go, s, c)

    tile = 256

    def serve_up(s, between=None):
        sums[...] = jnp.zeros(sums.shape, jnp.float32)
        for c in every:
            everyone(*go, s, c).wait_recv()
            block = arrived.at[s, c][...].reshape(slot_count, step)
            lines = slice(c * step, (c + 1) * step)
            for w, weight in enumerate((gate_w, up_w)):
                for f in range(ff // tile):
                    at = slice(f * tile, (f + 1) * tile)
                    to = slice(w * ff + f * tile, w * ff + (f + 1) * tile)
                    sums[:, to] += jnp.dot(block, weight[lines, at], preferred_element_type=jnp.float32)
            if between is not None:
                between(c)
        gate_value = sums[:, :ff]
        silu = gate_value * (1.0 / (1.0 + jnp.exp(-gate_value)))
        hidden[...] = (silu * sums[:, ff:]).astype(jnp.bfloat16)

    def serve_down(s, sends=None, between=None):
        for c in every:
            for f in range(step // tile):
                at = slice(c * step + f * tile, c * step + (f + 1) * tile)
                value = jnp.dot(hidden[...], down_w[:, at], preferred_element_type=jnp.float32)
                value = value.astype(jnp.bfloat16).reshape(group, cap, tile)
                served.at[s, c][:, :, f * tile : (f + 1) * tile] = value
            if sends is True:
                send_all(ret, s, c)
            elif sends is not None:
                pl.when(sends)(functools.partial(send_all, ret, s, c))
            if between is not None:
                between(c)

    def weighted(s, c):
        everyone(*ret, s, c).wait_recv()
        got = back.at[s, c][...].reshape(slot_count, step)
        return jnp.dot(high.at[s][...], got, preferred_element_type=jnp.float32) + jnp.dot(
            low.at[s][...], got, preferred_element_type=jnp.float32
        )

    def combine_own(c):
        carried_ref[:, c * step : (c + 1) * step] += weighted(z, c)

    def combine(j, c, slot):
        part_out.at[order[j], c][...] = weighted(order[j], c).astype(jnp.bfloat16)
        part_copy(order[j], c, slot, inner_z).start()

    def hold(j, c):
        held[j, c] = weighted(order[j], c)

    def relay(j, c, slot, level):
        part_copy(order[j], c, order[j], level).wait_recv()
        total = held[j, c] + part_in.at[order[j], c][...].astype(jnp.float32)
        part_out.at[order[j], c][...] = total.astype(jnp.bfloat16)
        part_copy(order[j], c, slot, level).start()

    def finish(c, arrivals):
        total = carried_ref[:, c * step : (c + 1) * step]
        for slot in arrivals:
            part_copy(z, c, slot, inner_z).wait_recv()
            total = total + part_in.at[slot, c][...].astype(jnp.float32)
        out_ref[:, c * step : (c + 1) * step] = total.astype(jnp.bfloat16)

    def all_sent(ref, sem):
        pltpu.make_async_remote_copy(
            src_ref=ref, dst_ref=ref, send_sem=sem, recv_sem=sem, device_id=homes[0], device_id_type=MESH
        ).wait_send()

    def slots_sent():
        all_sent(slots.at[:, :, pl.ds(0, group - 1)], go_send.at[0])
        all_sent(served.at[:, :, pl.ds(0, group - 1)], ret_send.at[0])
        all_sent(x_all.at[0], x_send.at[1])

    def slot_from(s, above):
        return s + (DEPTH - s) * above

    x_middle = (outer_z, inner_z, outer_z)
    lead = max(pieces // 4, 1)
    every = range(pieces)

    def quarter(first, last=None):
        last = first + 1 if last is None else last
        return range(first * pieces // 4, last * pieces // 4)

    for c in every:
        at = slice(c * step, (c + 1) * step)
        x_all.at[z, c][...] = (carried_ref[:, at] * scale * gain_ref[:, at]).astype(jnp.bfloat16)
        x_copy(1, z, c, inner_z).start()
        if c < lead:
            @pl.when(inward > 0)
            def _():
                x_copy(2, z, c, outer_z).start()
    for c in every:
        dispatch(z, c, own=True)
    for load in loads[10:13]:
        load.wait()

    def at_end(todo):
        pl.when(is_end)(todo)

    def in_middle(todo):
        pl.when(inward > 0)(todo)

    def meet(j, level=None):
        meta_copy(0, order[j], z).wait_recv()
        if level is not None:
            meta_copy(2 + j, order[j], level).start()
        choose(order[j])

    def arrive(j, *cs):
        for c in cs:
            if c == 0:
                meet(j)
            dispatch(order[j], c, None)

    def pass_on(j, *cs):
        for c in cs:
            if c == 0:
                meet(j, x_middle[j])
            dispatch(order[j], c, x_middle[j])

    def spread(*cs):
        for c in cs:
            pass_on(0, c)
            pass_on(1, c)

    def hooks(end, middle):
        def run(c):
            if c in end:
                at_end(end[c])
            if c in middle:
                in_middle(middle[c])

        return run

    def then(todo, *args):
        return functools.partial(todo, *args)

    def start_down():
        arrive(2, *range(lead))
        arrive(0, 0)

    in_middle(then(spread, 0))
    serve_up(
        z,
        hooks(
            {7: start_down},
            {0: then(spread, 1), 2: then(spread, 2), 4: then(spread, 3), 7: then(spread, 4)},
        ),
    )
    serve_down(z, None, hooks({3: then(arrive, 0, 1)}, {}))

    @at_end
    def _():
        for c in range(2, pieces):
            arrive(0, c)
            if c < pieces - 2:
                send_all(ret, z, c - 2)

    @in_middle
    def _():
        spread(5, 6, 7)

    serve_up(
        order[0],
        hooks(
            {6: then(arrive, 1, 0)},
            {3: then(pass_on, 2, 0), 5: then(pass_on, 2, 1), 6: then(pass_on, 2, 2)},
        ),
    )
    def send_back(j, *cs):
        for c in cs:
            send_all(ret, order[j], c)

    def both(first, second):
        def run():
            first()
            second()

        return run

    def reply(c):
        if c < 5:
            send_back(0, c)
        else:
            in_middle(then(send_back, 0, c))
        hooks(
            {1: then(arrive, 1, 1), 5: then(arrive, 1, 2)},
            {1: then(pass_on, 2, 3), 6: then(pass_on, 2, 4)},
        )(c)

    serve_down(order[0], None, reply)

    def hand_on(j, *cs):
        for c in cs:
            combine(j, c, order[j])

    @at_end
    def _():
        for c in range(3, 6):
            hand_on(0, c - 3)
            arrive(1, c)
            send_back(0, c + 2)
        hand_on(0, 3)
        arrive(1, 6)
        hand_on(0, 4)
        arrive(1, 7)
        hand_on(0, 5)

    serve_up(
        order[1],
        hooks(
            {3: then(hand_on, 0, 6), 5: then(hand_on, 0, 7)},
            {1: then(pass_on, 2, 5), 7: then(pass_on, 2, 6)},
        ),
    )

    serve_down(
        order[1],
        None,
        hooks(
            {
                0: then(send_back, 1, 0),
                1: both(then(send_back, 1, 1), then(arrive, 2, 2)),
                2: then(send_back, 1, 2),
                3: both(then(send_back, 1, 3), then(arrive, 2, 3)),
                5: then(arrive, 2, 4),
                7: then(arrive, 2, 5),
            },
            {3: then(pass_on, 2, 7)},
        ),
    )

    @at_end
    def _():
        arrive(2, 6)
        send_back(1, 4, 5)
        hand_on(1, 0)
        arrive(2, 7)
        send_back(1, 6, 7)
        hand_on(1, 1, 2, 3)

    @in_middle
    def _():
        for c in range(lead, pieces):
            x_copy(2, z, c, outer_z).start()
        for c in every:
            send_all(ret, order[1], c)
        for c in every:
            hold(0, c)

    @pl.when(has_next)
    def _():
        tail_copy(tp, lax.rem(sp + 1, sp_count)).wait_send()

    @pl.when(helps)
    def _():
        fix_copy(tp).wait_send()

    for b in range(tp_count):
        @pl.when(tp != b)
        def _():
            conv_copy(b, tp).wait_send()

    meta_copy(0, z, inner_z).wait_send()

    @pl.when(inward > 0)
    def _():
        meta_copy(1, z, outer_z).wait_send()
        for j in range(DEPTH - 1):
            meta_copy(2 + j, order[j], x_middle[j]).wait_send()

    serve_up(order[2], hooks({4: then(hand_on, 1, 4), 6: then(hand_on, 1, 5)}, {}))
    serve_down(order[2], True, hooks({3: then(hand_on, 1, 6), 7: then(hand_on, 1, 7)}, {}))

    @at_end
    def _():
        for c in range(pieces - 4, pieces):
            send_all(ret, z, c)
        for c in every:
            combine(2, c, slot_from(order[2], 1 - low_half))
        for c in every:
            combine_own(c)
        slots_sent()
        for c in every:
            finish(c, (slot_from(z, low_half),))

    @in_middle
    def _():
        to_middle = slot_from(order[0], 1 - low_half)
        to_end = slot_from(order[1], low_half)
        for c in every:
            send_all(ret, z, c)
        relay(0, 0, to_middle, inner_z)
        relay(0, 1, to_middle, inner_z)
        for c in every:
            hold(1, c)
        relay(0, 2, to_middle, inner_z)
        relay(0, 3, to_middle, inner_z)
        for c in range(4, pieces):
            relay(0, c, to_middle, inner_z)
            hold(2, 2 * c - 8)
            hold(2, 2 * c - 7)
        relay(2, 0, order[2], inner_z)
        for c in every:
            combine_own(c)
        for c in range(1, pieces + 2):
            if c < pieces:
                relay(2, c, order[2], inner_z)
            if c >= 2:
                relay(1, c - 2, to_end, outer_z)
        slots_sent()
        all_sent(x_all.at[pl.ds(0, DEPTH - 1)], x_send.at[0])
        all_sent(x_all.at[0], x_send.at[2])
        for c in every:
            finish(c, (z, DEPTH))

    all_sent(part_out.at[pl.ds(0, DEPTH - 1)], part_send.at[0])


def run_layer(front, routing, gate_proj, up_proj, down_proj, out_proj, cap, pieces=8):
    sp_count, tp_count = lax.axis_size("sp"), lax.axis_size("tp")
    length, channels = front[0].shape
    lanes = front[4].shape[1]
    rows, width = front[5].shape
    edge = 8
    ff = gate_proj.shape[2]
    group = sp_count // DEPTH * tp_count
    step = width // pieces
    slot_count = group * cap
    slot_shape = (DEPTH, pieces, group, cap, step)
    f32, bf16 = jnp.float32, jnp.bfloat16
    dma = pltpu.SemaphoreType.DMA
    vmem = pltpu.VMEM
    hbm = pl.BlockSpec(memory_space=pl.ANY)
    arrays = (*front, *routing)
    return pl.pallas_call(
        functools.partial(layer_kernel, sp_count, tp_count, cap, pieces),
        out_shape=pltpu.VMEM((rows, width), bf16),
        in_specs=[hbm] * (len(arrays) + 4),
        out_specs=pl.BlockSpec(memory_space=pltpu.VMEM),
        scratch_shapes=[vmem(a.shape, a.dtype) for a in arrays]
        + [
            vmem((width, ff), bf16),
            vmem((width, ff), bf16),
            vmem((ff, width), bf16),
            vmem(out_proj.shape, bf16),
            vmem((edge + length, channels), f32),
            vmem((edge + length, lanes), f32),
            vmem((edge, channels + lanes), f32),
            vmem((tp_count, edge, channels + lanes), f32),
            vmem((edge, channels), f32),
            vmem((tp_count, edge, channels), f32),
            vmem((tp_count, rows, channels), bf16),
            vmem((tp_count, rows, channels), bf16),
            vmem((rows, width), f32),
            vmem((DEPTH, 8, rows), f32),
            vmem((DEPTH, slot_count, rows), bf16),
            vmem((slot_count, rows), f32),
            vmem((DEPTH, rows, slot_count), bf16),
            vmem((DEPTH, rows, slot_count), bf16),
            vmem((DEPTH, pieces, rows, step), bf16),
            vmem(slot_shape, bf16),
            vmem(slot_shape, bf16),
            vmem(slot_shape, bf16),
            vmem(slot_shape, bf16),
            vmem((slot_count, ff), bf16),
            vmem((slot_count, 2 * ff), f32),
            vmem((DEPTH - 1, pieces, rows, step), f32),
            vmem((DEPTH, pieces, rows, step), bf16),
            vmem((DEPTH + 1, pieces, rows, step), bf16),
            dma((len(arrays) + 4,)),
            dma((1,)),
            dma((tp_count,)),
            dma((1,)),
            dma((tp_count,)),
            dma((tp_count,)),
            dma((tp_count,)),
            dma((DEPTH + 1,)),
            dma((DEPTH,)),
            dma((3,)),
            dma((DEPTH, pieces)),
            dma((1,)),
            dma((DEPTH, pieces)),
            dma((1,)),
            dma((DEPTH, pieces)),
            dma((1,)),
            dma((DEPTH + 1, pieces)),
        ],
        compiler_params=pltpu.CompilerParams(
            collective_id=0, has_side_effects=True, vmem_limit_bytes=56 * 1024 * 1024
        ),
    )(*arrays, gate_proj, up_proj, down_proj, out_proj)


def from_behind(block, axis, distance):
    devices = range(lax.axis_size(axis))
    route = [(i - distance, i) for i in devices if i - distance in devices]
    return lax.ppermute(block, axis, route)


def expert_rows(arrived, gate_weight, up_weight, down_weight):
    gate_value = jnp.dot(arrived, gate_weight, preferred_element_type=jnp.float32)
    up_value = jnp.dot(arrived, up_weight, preferred_element_type=jnp.float32)
    hidden = (jax.nn.silu(gate_value) * up_value).astype(jnp.bfloat16)
    return jnp.dot(hidden, down_weight, preferred_element_type=jnp.float32).astype(jnp.bfloat16)


def on_device(
    conv_input,
    gate_inner,
    gate_outer,
    conv_taps,
    doc_ids,
    residual_in,
    out_proj,
    norm_gain,
    expert_ids,
    expert_weights,
    gate_proj,
    up_proj,
    down_proj,
):
    sp_count, tp_count = lax.axis_size("sp"), lax.axis_size("tp")
    capacity = 2 * residual_in.shape[0] * expert_ids.shape[1] // (sp_count * tp_count)
    if capacity % 16 == 0 and sp_count % DEPTH == 0 and tp_count % 2 == 0:
        docs = doc_ids.reshape(-1, 128)
        front = (conv_input, gate_inner, gate_outer, conv_taps, docs, residual_in, norm_gain[None, :])
        routing = (expert_ids.T, expert_weights.T)
        return run_layer(front, routing, gate_proj, up_proj, down_proj, out_proj, capacity)
    inner_prod = conv_input.astype(jnp.float32) * gate_inner.astype(jnp.float32)
    earlier, earlier_docs = from_behind((inner_prod[-2:], doc_ids[-2:]), "sp", 1)
    padded = jnp.concatenate([earlier, inner_prod], axis=0)
    padded_docs = jnp.concatenate([earlier_docs, doc_ids], axis=0)
    length = inner_prod.shape[0]
    tap_values = conv_taps.astype(jnp.float32)
    one_back = jnp.where(
        (padded_docs[1 : length + 1] == doc_ids)[:, None], padded[1 : length + 1], 0.0
    )
    two_back = jnp.where((padded_docs[:length] == doc_ids)[:, None], padded[:length], 0.0)
    mixed_rows = tap_values[2] * inner_prod + tap_values[1] * one_back + tap_values[0] * two_back
    conv_out = (gate_outer.astype(jnp.float32) * mixed_rows).astype(jnp.bfloat16)
    row_count = residual_in.shape[0]
    regrouped = lax.all_to_all(conv_out, "tp", split_axis=0, concat_axis=1, tiled=True)
    mix = jnp.dot(regrouped, out_proj, preferred_element_type=jnp.float32).astype(jnp.bfloat16)
    carried = residual_in.astype(jnp.float32) + mix.astype(jnp.float32)
    normed = (
        carried * lax.rsqrt(jnp.mean(carried * carried, axis=1, keepdims=True) + 1e-06) * norm_gain
    ).astype(jnp.bfloat16)
    model_width = normed.shape[1]
    choose = expert_ids.shape[1]
    experts_total = sp_count * tp_count
    flat_ids = expert_ids.reshape(-1)
    onehot = (flat_ids[:, None] == jnp.arange(experts_total, dtype=jnp.int32)[None, :]).astype(
        jnp.int32
    )
    slot_rank = jnp.sum((jnp.cumsum(onehot, axis=0) - 1) * onehot, axis=1)
    target = flat_ids * capacity + slot_rank
    sources = jnp.repeat(normed, choose, axis=0)
    outgoing = (
        jnp.zeros((experts_total * capacity, model_width), jnp.bfloat16).at[target].set(sources)
    )
    gate_weight = gate_proj[0]
    up_weight = up_proj[0]
    down_weight = down_proj[0]
    arrived = lax.all_to_all(
        outgoing.reshape(experts_total, capacity, model_width),
        ("sp", "tp"),
        split_axis=0,
        concat_axis=0,
        tiled=True,
    )
    item_count = arrived.shape[1]
    flat_rows = arrived.reshape(-1, model_width)
    result = expert_rows(flat_rows, gate_weight, up_weight, down_weight)
    result = result.reshape(experts_total, item_count, model_width)
    returned = lax.all_to_all(result, ("sp", "tp"), split_axis=0, concat_axis=0, tiled=True)
    picked = (
        returned.reshape(-1, model_width)[target]
        .reshape(row_count, choose, model_width)
        .astype(jnp.float32)
    )
    combined = carried + jnp.sum(expert_weights[:, :, None] * picked, axis=1)
    return combined.astype(jnp.bfloat16)


def solution(mesh):
    in_specs = (
        P("sp", "tp"),
        P("sp", "tp"),
        P("sp", "tp"),
        P(None, "tp"),
        P("sp"),
        P(("sp", "tp"), None),
        P(),
        P(),
        P(("sp", "tp"), None),
        P(("sp", "tp"), None),
        P(("sp", "tp"), None, None),
        P(("sp", "tp"), None, None),
        P(("sp", "tp"), None, None),
    )
    out_specs = P(("sp", "tp"), None)
    return jax.shard_map(
        on_device, mesh=mesh, in_specs=in_specs, out_specs=out_specs, check_vma=False
    )
```

```python
import functools

import jax
import jax.numpy as jnp
from jax import lax
from jax.experimental import pallas as pl
from jax.experimental.pallas import tpu as pltpu
from jax.sharding import PartitionSpec as P

MESH = pl.DeviceIdType.MESH
DEPTH = 4


def layer_kernel(
    sp_count, tp_count, cap, pieces,
    conv_hbm, inner_hbm, outer_hbm, taps_hbm, docs_hbm, residual_hbm, gain_hbm, ids_hbm, scores_hbm,
    gate_hbm, up_hbm, down_hbm, proj_hbm,
    out_ref,
    conv_ref, inner_ref, outer_ref, taps_ref, docs_ref, residual_ref, gain_ref, ids_ref, scores_ref,
    gate_w, up_w, down_w, proj_w,
    padded, padded_docs, tail, tail_in, fix, fix_in, conv_out, conv_in, carried_ref,
    metas, place, wide, high, low, x_all, slots, arrived, served, back, hidden, sums, held, part_out, part_in,
    load_sem, tail_send, tail_recv, fix_send, fix_recv, conv_send, conv_recv, meta_send, meta_recv, x_send, x_recv,
    go_send, go_recv, ret_send, ret_recv, part_send, part_recv,
):
    sp = lax.axis_index("sp")
    tp = lax.axis_index("tp")
    span = sp_count // DEPTH
    group = span * tp_count
    z = lax.div(sp, span)
    y = lax.rem(sp, span)
    mine = y * tp_count + tp
    rows, width = carried_ref.shape
    step = width // pieces
    ff = gate_w.shape[1]
    slot_count = group * cap

    low_half = 1 - lax.div(z, DEPTH // 2)
    top = DEPTH - 1
    inward = z * low_half + (top - z) * (1 - low_half)
    is_end = inward == 0

    def flip(k):
        return k * low_half + (top - k) * (1 - low_half)

    def source(end, middle):
        return flip(end * (1 - inward) + middle * inward)

    order = (source(2, 2), source(3, 0), source(1, 3))
    outer_z, inner_z = flip(inward - 1), flip(inward + 1)

    def where(member):
        return (z * span + lax.div(member, tp_count), lax.rem(member, tp_count))

    def along(level):
        return (level * span + y, tp)

    pair = lax.div(tp, 2) * 2
    odd = tp - pair
    givers = [tp, pair + 1 - odd]
    for q in range(1, tp_count // 2):
        base = lax.rem(pair + 2 * q, tp_count)
        givers += [base + odd, base + 1 - odd]

    peers = []
    for i in range(span - 1, 0, -1):
        side = lax.rem(y + i, span) * tp_count
        peers += [side + t for t in givers[2:]]
    near = [lax.rem(y + i, span) * tp_count + t for i in range(1, span) for t in givers[:2]]
    here = [y * tp_count + t for t in givers[2:]]
    for i in range(max(len(near), len(here))):
        peers += near[i : i + 1] + here[i : i + 1]
    peers.append(y * tp_count + givers[1])
    homes = [where(other) for other in peers]

    pairs = (
        (conv_hbm, conv_ref), (inner_hbm, inner_ref), (docs_hbm, docs_ref), (taps_hbm, taps_ref), (outer_hbm, outer_ref),
        (ids_hbm, ids_ref), (scores_hbm, scores_ref), (residual_hbm, residual_ref), (gain_hbm, gain_ref),
        (proj_hbm, proj_w), (gate_hbm.at[0], gate_w), (up_hbm.at[0], up_w), (down_hbm.at[0], down_w),
    )
    loads = [
        pltpu.make_async_copy(origin, target, load_sem.at[n]) for n, (origin, target) in enumerate(pairs)
    ]
    for load in loads:
        load.start()

    barrier = pltpu.get_barrier_semaphore()
    for home in homes:
        pl.semaphore_signal(barrier, inc=1, device_id=home, device_id_type=MESH)
    pl.semaphore_signal(barrier, inc=1, device_id=along(inner_z), device_id_type=MESH)

    @pl.when(inward > 0)
    def _():
        pl.semaphore_signal(barrier, inc=1, device_id=along(outer_z), device_id_type=MESH)

    for t in range(tp_count):
        @pl.when((tp == 0) & (sp > 0))
        def _():
            pl.semaphore_signal(barrier, inc=1, device_id=(sp - 1, t), device_id_type=MESH)

    length, channels = conv_ref.shape
    lanes = tail.shape[1] - channels
    edge = tail.shape[0]
    for load in loads[:3]:
        load.wait()
    padded[edge:, :] = conv_ref[...].astype(jnp.float32) * inner_ref[...].astype(jnp.float32)
    docs = docs_ref[...].astype(jnp.float32)
    for j in range(length // lanes):
        at = slice(edge + j * lanes, edge + (j + 1) * lanes)
        padded_docs[at, :] = jnp.broadcast_to(docs[j : j + 1, :], (lanes, lanes)).T
    padded[:edge, :] = jnp.zeros((edge, channels), jnp.float32)
    padded_docs[:edge, :] = jnp.full((edge, lanes), -1.0, jnp.float32)
    tail[:, :channels] = padded[length:, :]
    tail[:, channels:] = padded_docs[length:, :]
    for load in loads[3:5]:
        load.wait()
    taps = taps_ref[...].astype(jnp.float32)

    def convolve(b):
        first = edge + b * rows
        docs = padded_docs[first : first + rows, :]
        same_one = padded_docs[first - 1 : first - 1 + rows, :] == docs
        same_two = padded_docs[first - 2 : first - 2 + rows, :] == docs
        for k in range(channels // lanes):
            at = slice(k * lanes, (k + 1) * lanes)
            one_back = jnp.where(same_one, padded[first - 1 : first - 1 + rows, at], 0.0)
            two_back = jnp.where(same_two, padded[first - 2 : first - 2 + rows, at], 0.0)
            here = padded[first : first + rows, at]
            mixed = taps[2:3, at] * here + taps[1:2, at] * one_back + taps[0:1, at] * two_back
            gated = outer_ref[b * rows : (b + 1) * rows, at].astype(jnp.float32) * mixed
            conv_out[b, :, at] = gated.astype(jnp.bfloat16)

    def conv_copy(b, landing):
        return pltpu.make_async_remote_copy(
            src_ref=conv_out.at[b], dst_ref=conv_in.at[landing],
            send_sem=conv_send.at[b], recv_sem=conv_recv.at[landing],
            device_id=(sp, b), device_id_type=MESH,
        )

    def hand_out(b):
        @pl.when(tp != b)
        def _():
            conv_copy(b, tp).start()

        @pl.when(tp == b)
        def _():
            conv_in[b] = conv_out[b]

    for k in range(channels // lanes):
        at = slice(k * lanes, (k + 1) * lanes)
        same_one = padded_docs[edge - 1 : 2 * edge - 1, :] == padded_docs[edge : 2 * edge, :]
        one_back = jnp.where(same_one, padded[edge - 1 : 2 * edge - 1, at], 0.0)
        mixed = taps[2:3, at] * padded[edge : 2 * edge, at] + taps[1:2, at] * one_back
        fix[0:2, at] = mixed[0:2]
    fix[2:4, :] = outer_ref[0:2, :].astype(jnp.float32)
    fix[4:6, :] = taps[0:2]
    fix[6:8, :] = jnp.zeros((2, channels), jnp.float32)

    for b in range(tp_count):
        convolve(b)
    for load in loads[5:7]:
        load.wait()
    metas.at[z][0:2, :] = ids_ref[...].astype(jnp.float32)
    metas.at[z][2:4, :] = scores_ref[...]
    metas.at[z][4:, :] = jnp.zeros((4, rows), jnp.float32)

    ahead = lax.div(2 * sp_count - 2 - sp, sp_count)
    pl.semaphore_wait(barrier, group + inward + ahead)

    def tail_copy(t, level):
        return pltpu.make_async_remote_copy(
            src_ref=tail, dst_ref=tail_in.at[t], send_sem=tail_send.at[0], recv_sem=tail_recv.at[t],
            device_id=(level, 0), device_id_type=MESH,
        )

    def fix_copy(t):
        return pltpu.make_async_remote_copy(
            src_ref=fix, dst_ref=fix_in.at[t], send_sem=fix_send.at[0], recv_sem=fix_recv.at[t],
            device_id=(sp, 0), device_id_type=MESH,
        )

    has_next = sp < sp_count - 1
    completes = (tp == 0) & (sp > 0)
    helps = (tp > 0) & (sp > 0)

    @pl.when(has_next)
    def _():
        tail_copy(tp, lax.rem(sp + 1, sp_count)).start()

    hand_out(0)

    @pl.when(helps)
    def _():
        fix_copy(tp).start()

    for b in range(1, tp_count):
        hand_out(b)

    @pl.when(completes)
    def _():
        fix_in[0] = fix[...]

    def complete(n):
        tail_copy(n, sp).wait_recv()
        if n > 0:
            fix_copy(n).wait_recv()
        line = lax.broadcasted_iota(jnp.int32, (16, lanes), 0)
        first_doc, second_doc = padded_docs[edge : edge + 1, :], padded_docs[edge + 1 : edge + 2, :]
        last_doc = tail_in[n, edge - 1 : edge, channels:]
        far_doc = tail_in[n, edge - 2 : edge - 1, channels:]
        for k in range(channels // lanes):
            at = slice(k * lanes, (k + 1) * lanes)
            last, far = tail_in[n, edge - 1 : edge, at], tail_in[n, edge - 2 : edge - 1, at]
            oldest, older = fix_in[n, 4:5, at], fix_in[n, 5:6, at]
            mixed = fix_in[n, 0:1, at] + older * jnp.where(last_doc == first_doc, last, 0.0)
            mixed = mixed + oldest * jnp.where(far_doc == first_doc, far, 0.0)
            row_zero = fix_in[n, 2:3, at] * mixed
            mixed = fix_in[n, 1:2, at] + oldest * jnp.where(last_doc == second_doc, last, 0.0)
            row_one = fix_in[n, 3:4, at] * mixed
            was = conv_in[n, 0:16, at].astype(jnp.float32)
            now = jnp.where(line == 0, row_zero, jnp.where(line == 1, row_one, was))
            conv_in[n, 0:16, at] = now.astype(jnp.bfloat16)


    def meta_copy(k, s, level):
        return pltpu.make_async_remote_copy(
            src_ref=metas.at[s], dst_ref=metas.at[s], send_sem=meta_send.at[k], recv_sem=meta_recv.at[s],
            device_id=along(level), device_id_type=MESH,
        )

    meta_copy(0, z, inner_z).start()

    @pl.when(inward > 0)
    def _():
        meta_copy(1, z, outer_z).start()

    first_expert = (z * group).astype(jnp.float32)
    ids = lax.broadcasted_iota(jnp.int32, (group, rows), 0).astype(jnp.float32) + first_expert
    earlier = lax.broadcasted_iota(jnp.int32, (rows, rows), 0) < lax.broadcasted_iota(jnp.int32, (rows, rows), 1)
    earlier = jnp.where(earlier, 1.0, 0.0).astype(jnp.bfloat16)
    seats = lax.broadcasted_iota(jnp.int32, (cap, rows), 0).astype(jnp.float32)

    def choose(s):
        meta = metas.at[s][...]
        taken = jnp.zeros((group, rows), jnp.float32)
        weight = jnp.zeros((group, rows), jnp.float32)
        for k in range(2):
            hit = meta[k : k + 1, :] == ids
            taken = taken + jnp.where(hit, 1.0, 0.0)
            weight = weight + jnp.where(hit, meta[2 + k : 3 + k, :], 0.0)
        rank = jnp.dot(taken.astype(jnp.bfloat16), earlier, preferred_element_type=jnp.float32)
        rank = jnp.where(taken > 0.5, rank, -1.0)
        for e in range(group):
            at = slice(e * cap, (e + 1) * cap)
            seated = rank[e : e + 1, :] == seats
            place.at[s][at, :] = jnp.where(seated, 1.0, 0.0).astype(jnp.bfloat16)
            wide[at, :] = jnp.where(seated, weight[e : e + 1, :], 0.0)
        total = wide[...].T
        upper = total.astype(jnp.bfloat16)
        high.at[s][...] = upper
        low.at[s][...] = (total - upper.astype(jnp.float32)).astype(jnp.bfloat16)

    choose(z)

    for load in loads[7:10]:
        load.wait()
    squares = jnp.zeros((rows, 1), jnp.float32)
    for n, giver in enumerate(givers):
        if n > 0:
            conv_copy(0, giver).wait_recv()

        @pl.when(completes)
        def _():
            complete(n)

        lines = pl.ds(pl.multiple_of(giver * channels, channels), channels)
        block = conv_in.at[giver][...]
        for c in range(pieces):
            at = slice(c * step, (c + 1) * step)
            mix = jnp.dot(block, proj_w[lines, at], preferred_element_type=jnp.float32)
            if n > 0:
                mix = carried_ref[:, at] + mix
            if n == tp_count - 1:
                mix = residual_ref[:, at].astype(jnp.float32) + mix.astype(jnp.bfloat16).astype(jnp.float32)
                squares = squares + jnp.sum(mix * mix, axis=1, keepdims=True)
            carried_ref[:, at] = mix
    scale = lax.rsqrt(squares / width + 1e-06)

    def x_copy(k, s, c, level):
        return pltpu.make_async_remote_copy(
            src_ref=x_all.at[s, c], dst_ref=x_all.at[s, c], send_sem=x_send.at[k], recv_sem=x_recv.at[s, c],
            device_id=along(level), device_id_type=MESH,
        )

    def part_copy(s, c, slot, level):
        return pltpu.make_async_remote_copy(
            src_ref=part_out.at[s, c], dst_ref=part_in.at[slot, c],
            send_sem=part_send.at[0], recv_sem=part_recv.at[slot, c],
            device_id=along(level), device_id_type=MESH,
        )

    def exchange(origin, target, send, recv, s, c, n):
        return pltpu.make_async_remote_copy(
            src_ref=origin.at[s, c, peers[n]], dst_ref=target.at[s, c, mine],
            send_sem=send.at[0], recv_sem=recv.at[s, c],
            device_id=homes[n], device_id_type=MESH,
        )

    def everyone(origin, target, send, recv, s, c):
        return pltpu.make_async_remote_copy(
            src_ref=origin.at[s, c, pl.ds(0, group - 1)], dst_ref=target.at[s, c, pl.ds(0, group - 1)],
            send_sem=send.at[0], recv_sem=recv.at[s, c],
            device_id=homes[0], device_id_type=MESH,
        )

    go = (slots, arrived, go_send, go_recv)
    ret = (served, back, ret_send, ret_recv)

    def send_all(way, s, c):
        for n in range(group - 1):
            exchange(*way, s, c, n).start()
        way[1].at[s, c, mine][...] = way[0].at[s, c, mine][...]

    def dispatch(s, c, level=None, own=False):
        if not own:
            x_copy(0, s, c, z).wait_recv()
        if level is not None:
            x_copy(0, s, c, level).start()
        picked = jnp.dot(place.at[s][...], x_all.at[s, c][...], preferred_element_type=jnp.float32)
        slots.at[s, c][...] = picked.astype(jnp.bfloat16).reshape(group, cap, step)
        send_all(go, s, c)

    tile = 256

    def serve_up(s, between=None):
        sums[...] = jnp.zeros(sums.shape, jnp.float32)
        for c in every:
            everyone(*go, s, c).wait_recv()
            block = arrived.at[s, c][...].reshape(slot_count, step)
            lines = slice(c * step, (c + 1) * step)
            for w, weight in enumerate((gate_w, up_w)):
                for f in range(ff // tile):
                    at = slice(f * tile, (f + 1) * tile)
                    to = slice(w * ff + f * tile, w * ff + (f + 1) * tile)
                    sums[:, to] += jnp.dot(block, weight[lines, at], preferred_element_type=jnp.float32)
            if between is not None:
                between(c)
        gate_value = sums[:, :ff]
        silu = gate_value * (1.0 / (1.0 + jnp.exp(-gate_value)))
        hidden[...] = (silu * sums[:, ff:]).astype(jnp.bfloat16)

    def serve_down(s, sends=None, between=None):
        for c in every:
            for f in range(step // tile):
                at = slice(c * step + f * tile, c * step + (f + 1) * tile)
                value = jnp.dot(hidden[...], down_w[:, at], preferred_element_type=jnp.float32)
                value = value.astype(jnp.bfloat16).reshape(group, cap, tile)
                served.at[s, c][:, :, f * tile : (f + 1) * tile] = value
            if sends is True:
                send_all(ret, s, c)
            elif sends is not None:
                pl.when(sends)(functools.partial(send_all, ret, s, c))
            if between is not None:
                between(c)

    def weighted(s, c):
        everyone(*ret, s, c).wait_recv()
        got = back.at[s, c][...].reshape(slot_count, step)
        return jnp.dot(high.at[s][...], got, preferred_element_type=jnp.float32) + jnp.dot(
            low.at[s][...], got, preferred_element_type=jnp.float32
        )

    def combine_own(c):
        carried_ref[:, c * step : (c + 1) * step] += weighted(z, c)

    def combine(j, c, slot):
        part_out.at[order[j], c][...] = weighted(order[j], c).astype(jnp.bfloat16)
        part_copy(order[j], c, slot, inner_z).start()

    def hold(j, c):
        held[j, c] = weighted(order[j], c)

    def relay(j, c, slot, level):
        part_copy(order[j], c, order[j], level).wait_recv()
        total = held[j, c] + part_in.at[order[j], c][...].astype(jnp.float32)
        part_out.at[order[j], c][...] = total.astype(jnp.bfloat16)
        part_copy(order[j], c, slot, level).start()

    def finish(c, arrivals):
        total = carried_ref[:, c * step : (c + 1) * step]
        for slot in arrivals:
            part_copy(z, c, slot, inner_z).wait_recv()
            total = total + part_in.at[slot, c][...].astype(jnp.float32)
        out_ref[:, c * step : (c + 1) * step] = total.astype(jnp.bfloat16)

    def all_sent(ref, sem):
        pltpu.make_async_remote_copy(
            src_ref=ref, dst_ref=ref, send_sem=sem, recv_sem=sem, device_id=homes[0], device_id_type=MESH
        ).wait_send()

    def slots_sent():
        all_sent(slots.at[:, :, pl.ds(0, group - 1)], go_send.at[0])
        all_sent(served.at[:, :, pl.ds(0, group - 1)], ret_send.at[0])
        all_sent(x_all.at[0], x_send.at[1])

    def slot_from(s, above):
        return s + (DEPTH - s) * above

    x_middle = (outer_z, inner_z, outer_z)
    lead = max(pieces // 4, 1)
    every = range(pieces)

    def quarter(first, last=None):
        last = first + 1 if last is None else last
        return range(first * pieces // 4, last * pieces // 4)

    for c in every:
        at = slice(c * step, (c + 1) * step)
        x_all.at[z, c][...] = (carried_ref[:, at] * scale * gain_ref[:, at]).astype(jnp.bfloat16)
        x_copy(1, z, c, inner_z).start()
        if c < lead:
            @pl.when(inward > 0)
            def _():
                x_copy(2, z, c, outer_z).start()
    for c in every:
        dispatch(z, c, own=True)
    for load in loads[10:13]:
        load.wait()

    def at_end(todo):
        pl.when(is_end)(todo)

    def in_middle(todo):
        pl.when(inward > 0)(todo)

    def meet(j, level=None):
        meta_copy(0, order[j], z).wait_recv()
        if level is not None:
            meta_copy(2 + j, order[j], level).start()
        choose(order[j])

    def arrive(j, *cs):
        for c in cs:
            if c == 0:
                meet(j)
            dispatch(order[j], c, None)

    def pass_on(j, *cs):
        for c in cs:
            if c == 0:
                meet(j, x_middle[j])
            dispatch(order[j], c, x_middle[j])

    def spread(*cs):
        for c in cs:
            pass_on(0, c)
            pass_on(1, c)

    def hooks(end, middle):
        def run(c):
            if c in end:
                at_end(end[c])
            if c in middle:
                in_middle(middle[c])

        return run

    def then(todo, *args):
        return functools.partial(todo, *args)

    def start_down():
        arrive(2, *range(lead))
        arrive(0, 0)

    in_middle(then(spread, 0))
    serve_up(
        z,
        hooks(
            {7: start_down},
            {0: then(spread, 1), 2: then(spread, 2), 4: then(spread, 3), 7: then(spread, 4)},
        ),
    )
    serve_down(z, None, hooks({3: then(arrive, 0, 1)}, {}))

    @at_end
    def _():
        for c in range(2, pieces):
            arrive(0, c)
            if c < pieces - 2:
                send_all(ret, z, c - 2)

    @in_middle
    def _():
        spread(5, 6, 7)

    serve_up(
        order[0],
        hooks(
            {6: then(arrive, 1, 0)},
            {3: then(pass_on, 2, 0), 5: then(pass_on, 2, 1), 6: then(pass_on, 2, 2)},
        ),
    )
    def send_back(j, *cs):
        for c in cs:
            send_all(ret, order[j], c)

    def both(first, second):
        def run():
            first()
            second()

        return run

    def reply(c):
        if c < 5:
            send_back(0, c)
        else:
            in_middle(then(send_back, 0, c))
        hooks(
            {1: then(arrive, 1, 1), 5: then(arrive, 1, 2)},
            {1: then(pass_on, 2, 3), 6: then(pass_on, 2, 4)},
        )(c)

    serve_down(order[0], None, reply)

    def hand_on(j, *cs):
        for c in cs:
            combine(j, c, order[j])

    @at_end
    def _():
        for c in range(3, pieces):
            hand_on(0, c - 3)
            arrive(1, c)
            if c == 3:
                send_back(0, 5)
        send_back(0, 6, 7)
        hand_on(0, 5)

    serve_up(
        order[1],
        hooks(
            {3: then(arrive, 2, 2), 6: then(arrive, 2, 3)},
            {1: then(pass_on, 2, 5), 7: then(pass_on, 2, 6)},
        ),
    )
    serve_down(
        order[1],
        None,
        hooks(
            {
                0: both(then(send_back, 1, 0), then(hand_on, 0, 6)),
                1: both(then(arrive, 2, 4), then(send_back, 1, 1)),
                2: both(then(send_back, 1, 2), then(hand_on, 0, 7)),
                3: then(send_back, 1, 3),
                5: then(arrive, 2, 5),
                7: then(send_back, 1, 4),
            },
            {3: then(pass_on, 2, 7)},
        ),
    )

    @at_end
    def _():
        arrive(2, 6)
        send_back(1, 5)
        hand_on(1, 0)
        arrive(2, 7)
        send_back(1, 6, 7)
        hand_on(1, 1, 2, 3)

    @in_middle
    def _():
        for c in range(lead, pieces):
            x_copy(2, z, c, outer_z).start()
        for c in every:
            send_all(ret, order[1], c)
        for c in every:
            hold(0, c)

    @pl.when(has_next)
    def _():
        tail_copy(tp, lax.rem(sp + 1, sp_count)).wait_send()

    @pl.when(helps)
    def _():
        fix_copy(tp).wait_send()

    for b in range(tp_count):
        @pl.when(tp != b)
        def _():
            conv_copy(b, tp).wait_send()

    meta_copy(0, z, inner_z).wait_send()

    @pl.when(inward > 0)
    def _():
        meta_copy(1, z, outer_z).wait_send()
        for j in range(DEPTH - 1):
            meta_copy(2 + j, order[j], x_middle[j]).wait_send()

    to_middle = slot_from(order[0], 1 - low_half)
    to_end = slot_from(order[1], low_half)

    def add_on(j, *cs):
        for c in cs:
            relay(j, c, to_middle, inner_z)

    serve_up(
        order[2],
        hooks(
            {4: then(hand_on, 1, 4), 6: then(hand_on, 1, 5)},
            {0: then(add_on, 0, 0), 4: then(add_on, 0, 1)},
        ),
    )
    serve_down(
        order[2],
        True,
        hooks(
            {3: then(hand_on, 1, 6), 7: then(hand_on, 1, 7)},
            {1: then(add_on, 0, 2), 5: then(add_on, 0, 3)},
        ),
    )

    @at_end
    def _():
        for c in range(pieces - 4, pieces):
            send_all(ret, z, c)
        for c in every:
            combine(2, c, slot_from(order[2], 1 - low_half))
        for c in every:
            combine_own(c)
        slots_sent()
        for c in every:
            finish(c, (slot_from(z, low_half),))

    @in_middle
    def _():
        for c in every:
            send_all(ret, z, c)
        add_on(0, 4)
        for c in every:
            hold(1, c)
        add_on(0, 5, 6)
        for c in every:
            hold(2, c)
            if c == 2:
                add_on(0, 7)
        relay(2, 0, order[2], inner_z)
        for c in range(1, pieces):
            relay(2, c, order[2], inner_z)
            if c >= 4:
                relay(1, c - 4, to_end, outer_z)
            combine_own(c - 1)
        combine_own(pieces - 1)
        for c in range(pieces - 4, pieces):
            relay(1, c, to_end, outer_z)
        slots_sent()
        all_sent(x_all.at[pl.ds(0, DEPTH - 1)], x_send.at[0])
        all_sent(x_all.at[0], x_send.at[2])
        for c in every:
            finish(c, (z, DEPTH))

    all_sent(part_out.at[pl.ds(0, DEPTH - 1)], part_send.at[0])


def run_layer(front, routing, gate_proj, up_proj, down_proj, out_proj, cap, pieces=8):
    sp_count, tp_count = lax.axis_size("sp"), lax.axis_size("tp")
    length, channels = front[0].shape
    lanes = front[4].shape[1]
    rows, width = front[5].shape
    edge = 8
    ff = gate_proj.shape[2]
    group = sp_count // DEPTH * tp_count
    step = width // pieces
    slot_count = group * cap
    slot_shape = (DEPTH, pieces, group, cap, step)
    f32, bf16 = jnp.float32, jnp.bfloat16
    dma = pltpu.SemaphoreType.DMA
    vmem = pltpu.VMEM
    hbm = pl.BlockSpec(memory_space=pl.ANY)
    arrays = (*front, *routing)
    return pl.pallas_call(
        functools.partial(layer_kernel, sp_count, tp_count, cap, pieces),
        out_shape=pltpu.VMEM((rows, width), bf16),
        in_specs=[hbm] * (len(arrays) + 4),
        out_specs=pl.BlockSpec(memory_space=pltpu.VMEM),
        scratch_shapes=[vmem(a.shape, a.dtype) for a in arrays]
        + [
            vmem((width, ff), bf16),
            vmem((width, ff), bf16),
            vmem((ff, width), bf16),
            vmem(out_proj.shape, bf16),
            vmem((edge + length, channels), f32),
            vmem((edge + length, lanes), f32),
            vmem((edge, channels + lanes), f32),
            vmem((tp_count, edge, channels + lanes), f32),
            vmem((edge, channels), f32),
            vmem((tp_count, edge, channels), f32),
            vmem((tp_count, rows, channels), bf16),
            vmem((tp_count, rows, channels), bf16),
            vmem((rows, width), f32),
            vmem((DEPTH, 8, rows), f32),
            vmem((DEPTH, slot_count, rows), bf16),
            vmem((slot_count, rows), f32),
            vmem((DEPTH, rows, slot_count), bf16),
            vmem((DEPTH, rows, slot_count), bf16),
            vmem((DEPTH, pieces, rows, step), bf16),
            vmem(slot_shape, bf16),
            vmem(slot_shape, bf16),
            vmem(slot_shape, bf16),
            vmem(slot_shape, bf16),
            vmem((slot_count, ff), bf16),
            vmem((slot_count, 2 * ff), f32),
            vmem((DEPTH - 1, pieces, rows, step), f32),
            vmem((DEPTH, pieces, rows, step), bf16),
            vmem((DEPTH + 1, pieces, rows, step), bf16),
            dma((len(arrays) + 4,)),
            dma((1,)),
            dma((tp_count,)),
            dma((1,)),
            dma((tp_count,)),
            dma((tp_count,)),
            dma((tp_count,)),
            dma((DEPTH + 1,)),
            dma((DEPTH,)),
            dma((3,)),
            dma((DEPTH, pieces)),
            dma((1,)),
            dma((DEPTH, pieces)),
            dma((1,)),
            dma((DEPTH, pieces)),
            dma((1,)),
            dma((DEPTH + 1, pieces)),
        ],
        compiler_params=pltpu.CompilerParams(
            collective_id=0, has_side_effects=True, vmem_limit_bytes=56 * 1024 * 1024
        ),
    )(*arrays, gate_proj, up_proj, down_proj, out_proj)


def from_behind(block, axis, distance):
    devices = range(lax.axis_size(axis))
    route = [(i - distance, i) for i in devices if i - distance in devices]
    return lax.ppermute(block, axis, route)


def expert_rows(arrived, gate_weight, up_weight, down_weight):
    gate_value = jnp.dot(arrived, gate_weight, preferred_element_type=jnp.float32)
    up_value = jnp.dot(arrived, up_weight, preferred_element_type=jnp.float32)
    hidden = (jax.nn.silu(gate_value) * up_value).astype(jnp.bfloat16)
    return jnp.dot(hidden, down_weight, preferred_element_type=jnp.float32).astype(jnp.bfloat16)


def on_device(
    conv_input,
    gate_inner,
    gate_outer,
    conv_taps,
    doc_ids,
    residual_in,
    out_proj,
    norm_gain,
    expert_ids,
    expert_weights,
    gate_proj,
    up_proj,
    down_proj,
):
    sp_count, tp_count = lax.axis_size("sp"), lax.axis_size("tp")
    capacity = 2 * residual_in.shape[0] * expert_ids.shape[1] // (sp_count * tp_count)
    if capacity % 16 == 0 and sp_count % DEPTH == 0 and tp_count % 2 == 0:
        docs = doc_ids.reshape(-1, 128)
        front = (conv_input, gate_inner, gate_outer, conv_taps, docs, residual_in, norm_gain[None, :])
        routing = (expert_ids.T, expert_weights.T)
        return run_layer(front, routing, gate_proj, up_proj, down_proj, out_proj, capacity)
    inner_prod = conv_input.astype(jnp.float32) * gate_inner.astype(jnp.float32)
    earlier, earlier_docs = from_behind((inner_prod[-2:], doc_ids[-2:]), "sp", 1)
    padded = jnp.concatenate([earlier, inner_prod], axis=0)
    padded_docs = jnp.concatenate([earlier_docs, doc_ids], axis=0)
    length = inner_prod.shape[0]
    tap_values = conv_taps.astype(jnp.float32)
    one_back = jnp.where(
        (padded_docs[1 : length + 1] == doc_ids)[:, None], padded[1 : length + 1], 0.0
    )
    two_back = jnp.where((padded_docs[:length] == doc_ids)[:, None], padded[:length], 0.0)
    mixed_rows = tap_values[2] * inner_prod + tap_values[1] * one_back + tap_values[0] * two_back
    conv_out = (gate_outer.astype(jnp.float32) * mixed_rows).astype(jnp.bfloat16)
    row_count = residual_in.shape[0]
    regrouped = lax.all_to_all(conv_out, "tp", split_axis=0, concat_axis=1, tiled=True)
    mix = jnp.dot(regrouped, out_proj, preferred_element_type=jnp.float32).astype(jnp.bfloat16)
    carried = residual_in.astype(jnp.float32) + mix.astype(jnp.float32)
    normed = (
        carried * lax.rsqrt(jnp.mean(carried * carried, axis=1, keepdims=True) + 1e-06) * norm_gain
    ).astype(jnp.bfloat16)
    model_width = normed.shape[1]
    choose = expert_ids.shape[1]
    experts_total = sp_count * tp_count
    flat_ids = expert_ids.reshape(-1)
    onehot = (flat_ids[:, None] == jnp.arange(experts_total, dtype=jnp.int32)[None, :]).astype(
        jnp.int32
    )
    slot_rank = jnp.sum((jnp.cumsum(onehot, axis=0) - 1) * onehot, axis=1)
    target = flat_ids * capacity + slot_rank
    sources = jnp.repeat(normed, choose, axis=0)
    outgoing = (
        jnp.zeros((experts_total * capacity, model_width), jnp.bfloat16).at[target].set(sources)
    )
    gate_weight = gate_proj[0]
    up_weight = up_proj[0]
    down_weight = down_proj[0]
    arrived = lax.all_to_all(
        outgoing.reshape(experts_total, capacity, model_width),
        ("sp", "tp"),
        split_axis=0,
        concat_axis=0,
        tiled=True,
    )
    item_count = arrived.shape[1]
    flat_rows = arrived.reshape(-1, model_width)
    result = expert_rows(flat_rows, gate_weight, up_weight, down_weight)
    result = result.reshape(experts_total, item_count, model_width)
    returned = lax.all_to_all(result, ("sp", "tp"), split_axis=0, concat_axis=0, tiled=True)
    picked = (
        returned.reshape(-1, model_width)[target]
        .reshape(row_count, choose, model_width)
        .astype(jnp.float32)
    )
    combined = carried + jnp.sum(expert_weights[:, :, None] * picked, axis=1)
    return combined.astype(jnp.bfloat16)


def solution(mesh):
    in_specs = (
        P("sp", "tp"),
        P("sp", "tp"),
        P("sp", "tp"),
        P(None, "tp"),
        P("sp"),
        P(("sp", "tp"), None),
        P(),
        P(),
        P(("sp", "tp"), None),
        P(("sp", "tp"), None),
        P(("sp", "tp"), None, None),
        P(("sp", "tp"), None, None),
        P(("sp", "tp"), None, None),
    )
    out_specs = P(("sp", "tp"), None)
    return jax.shard_map(
        on_device, mesh=mesh, in_specs=in_specs, out_specs=out_specs, check_vma=False
    )
```

```python
import functools

import jax
import jax.numpy as jnp
from jax import lax
from jax.experimental import pallas as pl
from jax.experimental.pallas import tpu as pltpu
from jax.sharding import PartitionSpec as P

MESH = pl.DeviceIdType.MESH
DEPTH = 4


def layer_kernel(
    sp_count, tp_count, cap, pieces,
    conv_hbm, inner_hbm, outer_hbm, taps_hbm, docs_hbm, residual_hbm, gain_hbm, ids_hbm, scores_hbm,
    gate_hbm, up_hbm, down_hbm, proj_hbm,
    out_ref,
    conv_ref, inner_ref, outer_ref, taps_ref, docs_ref, residual_ref, gain_ref, ids_ref, scores_ref,
    gate_w, up_w, down_w, proj_w,
    padded, padded_docs, tail, tail_in, fix, fix_in, conv_out, conv_in, carried_ref,
    metas, place, wide, high, low, x_all, slots, arrived, served, back, hidden, sums, held, part_out, part_in,
    load_sem, tail_send, tail_recv, fix_send, fix_recv, conv_send, conv_recv, meta_send, meta_recv, x_send, x_recv,
    go_send, go_recv, ret_send, part_send, part_recv,
):
    sp = lax.axis_index("sp")
    tp = lax.axis_index("tp")
    span = sp_count // DEPTH
    group = span * tp_count
    z = lax.div(sp, span)
    y = lax.rem(sp, span)
    mine = y * tp_count + tp
    rows, width = carried_ref.shape
    step = width // pieces
    ff = gate_w.shape[1]
    slot_count = group * cap

    low_half = 1 - lax.div(z, DEPTH // 2)
    top = DEPTH - 1
    inward = z * low_half + (top - z) * (1 - low_half)
    is_end = inward == 0

    def flip(k):
        return k * low_half + (top - k) * (1 - low_half)

    def source(end, middle):
        return flip(end * (1 - inward) + middle * inward)

    order = (source(2, 2), source(3, 0), source(1, 3))
    outer_z, inner_z = flip(inward - 1), flip(inward + 1)

    def where(member):
        return (z * span + lax.div(member, tp_count), lax.rem(member, tp_count))

    def along(level):
        return (level * span + y, tp)

    pair = lax.div(tp, 2) * 2
    odd = tp - pair
    givers = [tp, pair + 1 - odd]
    for q in range(1, tp_count // 2):
        base = lax.rem(pair + 2 * q, tp_count)
        givers += [base + odd, base + 1 - odd]

    peers = []
    for i in range(span - 1, 0, -1):
        side = lax.rem(y + i, span) * tp_count
        peers += [side + t for t in givers[2:]]
    near = [lax.rem(y + i, span) * tp_count + t for i in range(1, span) for t in givers[:2]]
    here = [y * tp_count + t for t in givers[2:]]
    for i in range(max(len(near), len(here))):
        peers += near[i : i + 1] + here[i : i + 1]
    peers.append(y * tp_count + givers[1])
    homes = [where(other) for other in peers]

    pairs = (
        (conv_hbm, conv_ref), (inner_hbm, inner_ref), (docs_hbm, docs_ref), (taps_hbm, taps_ref), (outer_hbm, outer_ref),
        (ids_hbm, ids_ref), (scores_hbm, scores_ref), (residual_hbm, residual_ref), (gain_hbm, gain_ref),
        (proj_hbm, proj_w), (gate_hbm.at[0], gate_w), (up_hbm.at[0], up_w), (down_hbm.at[0], down_w),
    )
    loads = [
        pltpu.make_async_copy(origin, target, load_sem.at[n]) for n, (origin, target) in enumerate(pairs)
    ]
    for load in loads:
        load.start()

    barrier = pltpu.get_barrier_semaphore()
    for home in homes:
        pl.semaphore_signal(barrier, inc=1, device_id=home, device_id_type=MESH)
    pl.semaphore_signal(barrier, inc=1, device_id=along(inner_z), device_id_type=MESH)

    @pl.when(inward > 0)
    def _():
        pl.semaphore_signal(barrier, inc=1, device_id=along(outer_z), device_id_type=MESH)

    for t in range(tp_count):
        @pl.when((tp == 0) & (sp > 0))
        def _():
            pl.semaphore_signal(barrier, inc=1, device_id=(sp - 1, t), device_id_type=MESH)

    length, channels = conv_ref.shape
    lanes = tail.shape[1] - channels
    edge = tail.shape[0]
    for load in loads[:3]:
        load.wait()
    padded[edge:, :] = conv_ref[...].astype(jnp.float32) * inner_ref[...].astype(jnp.float32)
    docs = docs_ref[...].astype(jnp.float32)
    for j in range(length // lanes):
        at = slice(edge + j * lanes, edge + (j + 1) * lanes)
        padded_docs[at, :] = jnp.broadcast_to(docs[j : j + 1, :], (lanes, lanes)).T
    padded[:edge, :] = jnp.zeros((edge, channels), jnp.float32)
    padded_docs[:edge, :] = jnp.full((edge, lanes), -1.0, jnp.float32)
    tail[:, :channels] = padded[length:, :]
    tail[:, channels:] = padded_docs[length:, :]
    for load in loads[3:5]:
        load.wait()
    taps = taps_ref[...].astype(jnp.float32)

    def convolve(b):
        first = edge + b * rows
        docs = padded_docs[first : first + rows, :]
        same_one = padded_docs[first - 1 : first - 1 + rows, :] == docs
        same_two = padded_docs[first - 2 : first - 2 + rows, :] == docs
        for k in range(channels // lanes):
            at = slice(k * lanes, (k + 1) * lanes)
            one_back = jnp.where(same_one, padded[first - 1 : first - 1 + rows, at], 0.0)
            two_back = jnp.where(same_two, padded[first - 2 : first - 2 + rows, at], 0.0)
            here = padded[first : first + rows, at]
            mixed = taps[2:3, at] * here + taps[1:2, at] * one_back + taps[0:1, at] * two_back
            gated = outer_ref[b * rows : (b + 1) * rows, at].astype(jnp.float32) * mixed
            conv_out[b, :, at] = gated.astype(jnp.bfloat16)

    def conv_copy(b, landing):
        return pltpu.make_async_remote_copy(
            src_ref=conv_out.at[b], dst_ref=conv_in.at[landing],
            send_sem=conv_send.at[b], recv_sem=conv_recv.at[landing],
            device_id=(sp, b), device_id_type=MESH,
        )

    def hand_out(b):
        @pl.when(tp != b)
        def _():
            conv_copy(b, tp).start()

        @pl.when(tp == b)
        def _():
            conv_in[b] = conv_out[b]

    for k in range(channels // lanes):
        at = slice(k * lanes, (k + 1) * lanes)
        same_one = padded_docs[edge - 1 : 2 * edge - 1, :] == padded_docs[edge : 2 * edge, :]
        one_back = jnp.where(same_one, padded[edge - 1 : 2 * edge - 1, at], 0.0)
        mixed = taps[2:3, at] * padded[edge : 2 * edge, at] + taps[1:2, at] * one_back
        fix[0:2, at] = mixed[0:2]
    fix[2:4, :] = outer_ref[0:2, :].astype(jnp.float32)
    fix[4:6, :] = taps[0:2]
    fix[6:8, :] = jnp.zeros((2, channels), jnp.float32)

    for b in range(tp_count):
        convolve(b)
    for load in loads[5:7]:
        load.wait()
    metas.at[z][0:2, :] = ids_ref[...].astype(jnp.float32)
    metas.at[z][2:4, :] = scores_ref[...]
    metas.at[z][4:, :] = jnp.zeros((4, rows), jnp.float32)

    ahead = lax.div(2 * sp_count - 2 - sp, sp_count)
    pl.semaphore_wait(barrier, group + inward + ahead)

    def tail_copy(t, level):
        return pltpu.make_async_remote_copy(
            src_ref=tail, dst_ref=tail_in.at[t], send_sem=tail_send.at[0], recv_sem=tail_recv.at[t],
            device_id=(level, 0), device_id_type=MESH,
        )

    def fix_copy(t):
        return pltpu.make_async_remote_copy(
            src_ref=fix, dst_ref=fix_in.at[t], send_sem=fix_send.at[0], recv_sem=fix_recv.at[t],
            device_id=(sp, 0), device_id_type=MESH,
        )

    has_next = sp < sp_count - 1
    completes = (tp == 0) & (sp > 0)
    helps = (tp > 0) & (sp > 0)

    @pl.when(has_next)
    def _():
        tail_copy(tp, lax.rem(sp + 1, sp_count)).start()

    hand_out(0)

    @pl.when(helps)
    def _():
        fix_copy(tp).start()

    for b in range(1, tp_count):
        hand_out(b)

    @pl.when(completes)
    def _():
        fix_in[0] = fix[...]

    def complete(n):
        tail_copy(n, sp).wait_recv()
        if n > 0:
            fix_copy(n).wait_recv()
        line = lax.broadcasted_iota(jnp.int32, (16, lanes), 0)
        first_doc, second_doc = padded_docs[edge : edge + 1, :], padded_docs[edge + 1 : edge + 2, :]
        last_doc = tail_in[n, edge - 1 : edge, channels:]
        far_doc = tail_in[n, edge - 2 : edge - 1, channels:]
        for k in range(channels // lanes):
            at = slice(k * lanes, (k + 1) * lanes)
            last, far = tail_in[n, edge - 1 : edge, at], tail_in[n, edge - 2 : edge - 1, at]
            oldest, older = fix_in[n, 4:5, at], fix_in[n, 5:6, at]
            mixed = fix_in[n, 0:1, at] + older * jnp.where(last_doc == first_doc, last, 0.0)
            mixed = mixed + oldest * jnp.where(far_doc == first_doc, far, 0.0)
            row_zero = fix_in[n, 2:3, at] * mixed
            mixed = fix_in[n, 1:2, at] + oldest * jnp.where(last_doc == second_doc, last, 0.0)
            row_one = fix_in[n, 3:4, at] * mixed
            was = conv_in[n, 0:16, at].astype(jnp.float32)
            now = jnp.where(line == 0, row_zero, jnp.where(line == 1, row_one, was))
            conv_in[n, 0:16, at] = now.astype(jnp.bfloat16)


    def meta_copy(k, s, level):
        return pltpu.make_async_remote_copy(
            src_ref=metas.at[s], dst_ref=metas.at[s], send_sem=meta_send.at[k], recv_sem=meta_recv.at[s],
            device_id=along(level), device_id_type=MESH,
        )

    meta_copy(0, z, inner_z).start()

    @pl.when(inward > 0)
    def _():
        meta_copy(1, z, outer_z).start()

    first_expert = (z * group).astype(jnp.float32)
    ids = lax.broadcasted_iota(jnp.int32, (group, rows), 0).astype(jnp.float32) + first_expert
    earlier = lax.broadcasted_iota(jnp.int32, (rows, rows), 0) < lax.broadcasted_iota(jnp.int32, (rows, rows), 1)
    earlier = jnp.where(earlier, 1.0, 0.0).astype(jnp.bfloat16)
    seats = lax.broadcasted_iota(jnp.int32, (cap, rows), 0).astype(jnp.float32)

    def choose(s):
        meta = metas.at[s][...]
        taken = jnp.zeros((group, rows), jnp.float32)
        weight = jnp.zeros((group, rows), jnp.float32)
        for k in range(2):
            hit = meta[k : k + 1, :] == ids
            taken = taken + jnp.where(hit, 1.0, 0.0)
            weight = weight + jnp.where(hit, meta[2 + k : 3 + k, :], 0.0)
        rank = jnp.dot(taken.astype(jnp.bfloat16), earlier, preferred_element_type=jnp.float32)
        rank = jnp.where(taken > 0.5, rank, -1.0)
        for e in range(group):
            at = slice(e * cap, (e + 1) * cap)
            seated = rank[e : e + 1, :] == seats
            place.at[s][at, :] = jnp.where(seated, 1.0, 0.0).astype(jnp.bfloat16)
            wide[at, :] = jnp.where(seated, weight[e : e + 1, :], 0.0)
        total = wide[...].T
        upper = total.astype(jnp.bfloat16)
        high.at[s][...] = upper
        low.at[s][...] = (total - upper.astype(jnp.float32)).astype(jnp.bfloat16)

    choose(z)

    for load in loads[7:10]:
        load.wait()
    squares = jnp.zeros((rows, 1), jnp.float32)
    for n, giver in enumerate(givers):
        if n > 0:
            conv_copy(0, giver).wait_recv()

        @pl.when(completes)
        def _():
            complete(n)

        lines = pl.ds(pl.multiple_of(giver * channels, channels), channels)
        block = conv_in.at[giver][...]
        for c in range(pieces):
            at = slice(c * step, (c + 1) * step)
            mix = jnp.dot(block, proj_w[lines, at], preferred_element_type=jnp.float32)
            if n > 0:
                mix = carried_ref[:, at] + mix
            if n == tp_count - 1:
                mix = residual_ref[:, at].astype(jnp.float32) + mix.astype(jnp.bfloat16).astype(jnp.float32)
                squares = squares + jnp.sum(mix * mix, axis=1, keepdims=True)
            carried_ref[:, at] = mix
    scale = lax.rsqrt(squares / width + 1e-06)

    def x_copy(k, s, c, level):
        return pltpu.make_async_remote_copy(
            src_ref=x_all.at[s, c], dst_ref=x_all.at[s, c], send_sem=x_send.at[k], recv_sem=x_recv.at[s, c],
            device_id=along(level), device_id_type=MESH,
        )

    def part_copy(s, c, slot, level):
        return pltpu.make_async_remote_copy(
            src_ref=part_out.at[s, c], dst_ref=part_in.at[slot, c],
            send_sem=part_send.at[0], recv_sem=part_recv.at[slot, c],
            device_id=along(level), device_id_type=MESH,
        )

    def exchange(origin, target, send, recv, s, c, n):
        return pltpu.make_async_remote_copy(
            src_ref=origin.at[s, c, peers[n]], dst_ref=target.at[s, c, mine],
            send_sem=send.at[0], recv_sem=recv.at[s, c],
            device_id=homes[n], device_id_type=MESH,
        )

    def everyone(origin, target, send, recv, s, c):
        return pltpu.make_async_remote_copy(
            src_ref=origin.at[s, c, pl.ds(0, group - 1)], dst_ref=target.at[s, c, pl.ds(0, group - 1)],
            send_sem=send.at[0], recv_sem=recv.at[s, c],
            device_id=homes[0], device_id_type=MESH,
        )

    go = (slots, arrived, go_send, go_recv)
    ret = (served, back, ret_send, x_recv)

    def send_all(way, s, c):
        for n in range(group - 1):
            exchange(*way, s, c, n).start()
        way[1].at[s, c, mine][...] = way[0].at[s, c, mine][...]

    def dispatch(s, c, level=None, own=False):
        if not own:
            x_copy(0, s, c, z).wait_recv()
        if level is not None:
            x_copy(0, s, c, level).start()
        picked = jnp.dot(place.at[s][...], x_all.at[s, c][...], preferred_element_type=jnp.float32)
        slots.at[s, c][...] = picked.astype(jnp.bfloat16).reshape(group, cap, step)
        send_all(go, s, c)

    tile = 256

    def serve_up(s, between=None):
        sums[...] = jnp.zeros(sums.shape, jnp.float32)
        for c in every:
            everyone(*go, s, c).wait_recv()
            block = arrived.at[s, c][...].reshape(slot_count, step)
            lines = slice(c * step, (c + 1) * step)
            for w, weight in enumerate((gate_w, up_w)):
                for f in range(ff // tile):
                    at = slice(f * tile, (f + 1) * tile)
                    to = slice(w * ff + f * tile, w * ff + (f + 1) * tile)
                    sums[:, to] += jnp.dot(block, weight[lines, at], preferred_element_type=jnp.float32)
            if between is not None:
                between(c)
        gate_value = sums[:, :ff]
        silu = gate_value * (1.0 / (1.0 + jnp.exp(-gate_value)))
        hidden[...] = (silu * sums[:, ff:]).astype(jnp.bfloat16)

    def serve_down(s, sends=None, between=None):
        for c in every:
            for f in range(step // tile):
                at = slice(c * step + f * tile, c * step + (f + 1) * tile)
                value = jnp.dot(hidden[...], down_w[:, at], preferred_element_type=jnp.float32)
                value = value.astype(jnp.bfloat16).reshape(group, cap, tile)
                served.at[s, c][:, :, f * tile : (f + 1) * tile] = value
            if sends is True:
                send_all(ret, s, c)
            elif sends is not None:
                pl.when(sends)(functools.partial(send_all, ret, s, c))
            if between is not None:
                between(c)

    def weighted(s, c):
        everyone(*ret, s, c).wait_recv()
        got = back.at[s, c][...].reshape(slot_count, step)
        return jnp.dot(high.at[s][...], got, preferred_element_type=jnp.float32) + jnp.dot(
            low.at[s][...], got, preferred_element_type=jnp.float32
        )

    def combine_own(c):
        carried_ref[:, c * step : (c + 1) * step] += weighted(z, c)

    def combine(j, c, slot):
        part_out.at[order[j], c][...] = weighted(order[j], c).astype(jnp.bfloat16)
        part_copy(order[j], c, slot, inner_z).start()

    def hold(j, c):
        held[j, c] = weighted(order[j], c)

    def relay(j, c, slot, level):
        part_copy(order[j], c, order[j], level).wait_recv()
        total = held[j, c] + part_in.at[order[j], c][...].astype(jnp.float32)
        part_out.at[order[j], c][...] = total.astype(jnp.bfloat16)
        part_copy(order[j], c, slot, level).start()

    def finish(c, arrivals):
        total = carried_ref[:, c * step : (c + 1) * step]
        for slot in arrivals:
            part_copy(z, c, slot, inner_z).wait_recv()
            total = total + part_in.at[slot, c][...].astype(jnp.float32)
        out_ref[:, c * step : (c + 1) * step] = total.astype(jnp.bfloat16)

    def all_sent(ref, sem):
        pltpu.make_async_remote_copy(
            src_ref=ref, dst_ref=ref, send_sem=sem, recv_sem=sem, device_id=homes[0], device_id_type=MESH
        ).wait_send()

    def slots_sent():
        all_sent(slots.at[:, :, pl.ds(0, group - 1)], go_send.at[0])
        all_sent(served.at[:, :, pl.ds(0, group - 1)], ret_send.at[0])
        all_sent(x_all.at[0], x_send.at[1])

    def slot_from(s, above):
        return s + (DEPTH - s) * above

    x_middle = (outer_z, inner_z, outer_z)
    lead = max(pieces // 4, 1)
    every = range(pieces)

    def quarter(first, last=None):
        last = first + 1 if last is None else last
        return range(first * pieces // 4, last * pieces // 4)

    for c in every:
        at = slice(c * step, (c + 1) * step)
        x_all.at[z, c][...] = (carried_ref[:, at] * scale * gain_ref[:, at]).astype(jnp.bfloat16)
        x_copy(1, z, c, inner_z).start()
        if c < lead:
            @pl.when(inward > 0)
            def _():
                x_copy(2, z, c, outer_z).start()
    for c in every:
        dispatch(z, c, own=True)
    for load in loads[10:13]:
        load.wait()

    def at_end(todo):
        pl.when(is_end)(todo)

    def in_middle(todo):
        pl.when(inward > 0)(todo)

    def meet(j, level=None):
        meta_copy(0, order[j], z).wait_recv()
        if level is not None:
            meta_copy(2 + j, order[j], level).start()
        choose(order[j])

    def arrive(j, *cs):
        for c in cs:
            if c == 0:
                meet(j)
            dispatch(order[j], c, None)

    def pass_on(j, *cs):
        for c in cs:
            if c == 0:
                meet(j, x_middle[j])
            dispatch(order[j], c, x_middle[j])

    def spread(*cs):
        for c in cs:
            pass_on(0, c)
            pass_on(1, c)

    def hooks(end, middle):
        def run(c):
            if c in end:
                at_end(end[c])
            if c in middle:
                in_middle(middle[c])

        return run

    def then(todo, *args):
        return functools.partial(todo, *args)

    def start_down():
        arrive(2, *range(lead))
        arrive(0, 0)

    in_middle(then(spread, 0))
    serve_up(
        z,
        hooks(
            {7: start_down},
            {0: then(spread, 1), 2: then(spread, 2), 4: then(spread, 3), 7: then(spread, 4)},
        ),
    )
    serve_down(z, None, hooks({3: then(arrive, 0, 1)}, {}))

    @at_end
    def _():
        for c in range(2, pieces):
            arrive(0, c)
            if c < pieces - 2:
                send_all(ret, z, c - 2)

    @in_middle
    def _():
        spread(5, 6, 7)

    serve_up(
        order[0],
        hooks(
            {6: then(arrive, 1, 0)},
            {3: then(pass_on, 2, 0), 5: then(pass_on, 2, 1), 6: then(pass_on, 2, 2)},
        ),
    )
    def send_back(j, *cs):
        for c in cs:
            send_all(ret, order[j], c)

    def both(first, second):
        def run():
            first()
            second()

        return run

    def reply(c):
        if c < 5:
            send_back(0, c)
        else:
            in_middle(then(send_back, 0, c))
        hooks(
            {1: then(arrive, 1, 1), 5: then(arrive, 1, 2)},
            {1: then(pass_on, 2, 3), 6: then(pass_on, 2, 4)},
        )(c)

    serve_down(order[0], None, reply)

    def hand_on(j, *cs):
        for c in cs:
            combine(j, c, order[j])

    @at_end
    def _():
        for c in range(3, pieces):
            hand_on(0, c - 3)
            arrive(1, c)
            if c == 3:
                send_back(0, 5)
        send_back(0, 6, 7)
        hand_on(0, 5)

    serve_up(
        order[1],
        hooks(
            {3: then(arrive, 2, 2)},
            {1: then(pass_on, 2, 5), 7: then(pass_on, 2, 6)},
        ),
    )
    serve_down(
        order[1],
        None,
        hooks(
            {
                0: both(then(send_back, 1, 0), then(hand_on, 0, 6)),
                1: both(then(arrive, 2, 3, 4), then(send_back, 1, 1)),
                2: both(then(send_back, 1, 2), then(hand_on, 0, 7)),
                3: then(send_back, 1, 3),
                5: then(arrive, 2, 5),
                7: then(send_back, 1, 4),
            },
            {3: then(pass_on, 2, 7)},
        ),
    )

    @at_end
    def _():
        arrive(2, 6)
        send_back(1, 5)
        hand_on(1, 0)
        arrive(2, 7)
        send_back(1, 6, 7)
        hand_on(1, 1, 2, 3)

    @in_middle
    def _():
        for c in range(lead, pieces):
            x_copy(2, z, c, outer_z).start()
        for c in every:
            send_all(ret, order[1], c)
        for c in every:
            hold(0, c)

    @pl.when(has_next)
    def _():
        tail_copy(tp, lax.rem(sp + 1, sp_count)).wait_send()

    @pl.when(helps)
    def _():
        fix_copy(tp).wait_send()

    for b in range(tp_count):
        @pl.when(tp != b)
        def _():
            conv_copy(b, tp).wait_send()

    meta_copy(0, z, inner_z).wait_send()

    @pl.when(inward > 0)
    def _():
        meta_copy(1, z, outer_z).wait_send()
        for j in range(DEPTH - 1):
            meta_copy(2 + j, order[j], x_middle[j]).wait_send()

    to_middle = slot_from(order[0], 1 - low_half)
    to_end = slot_from(order[1], low_half)

    def add_on(j, *cs):
        for c in cs:
            relay(j, c, to_middle, inner_z)

    serve_up(
        order[2],
        hooks(
            {4: then(hand_on, 1, 4), 6: then(hand_on, 1, 5)},
            {0: then(add_on, 0, 0), 4: then(add_on, 0, 1)},
        ),
    )
    serve_down(
        order[2],
        True,
        hooks(
            {3: then(hand_on, 1, 6), 7: then(hand_on, 1, 7)},
            {1: then(add_on, 0, 2), 5: then(add_on, 0, 3)},
        ),
    )

    @at_end
    def _():
        for c in range(pieces - 4, pieces):
            send_all(ret, z, c)
        for c in every:
            combine(2, c, slot_from(order[2], 1 - low_half))
        for c in every:
            combine_own(c)
        slots_sent()
        for c in every:
            finish(c, (slot_from(z, low_half),))

    @in_middle
    def _():
        for c in every:
            send_all(ret, z, c)
        add_on(0, 4)
        for c in every:
            hold(1, c)
        add_on(0, 5, 6)
        for c in every:
            hold(2, c)
            if c == 2:
                add_on(0, 7)
        relay(2, 0, order[2], inner_z)
        for c in range(1, pieces):
            relay(2, c, order[2], inner_z)
            if c >= 4:
                relay(1, c - 4, to_end, outer_z)
            combine_own(c - 1)
        combine_own(pieces - 1)
        for c in range(pieces - 4, pieces):
            relay(1, c, to_end, outer_z)
        slots_sent()
        all_sent(x_all.at[pl.ds(0, DEPTH - 1)], x_send.at[0])
        all_sent(x_all.at[0], x_send.at[2])
        for c in every:
            finish(c, (z, DEPTH))

    all_sent(part_out.at[pl.ds(0, DEPTH - 1)], part_send.at[0])


def run_layer(front, routing, gate_proj, up_proj, down_proj, out_proj, cap, pieces=8):
    sp_count, tp_count = lax.axis_size("sp"), lax.axis_size("tp")
    length, channels = front[0].shape
    lanes = front[4].shape[1]
    rows, width = front[5].shape
    edge = 8
    ff = gate_proj.shape[2]
    group = sp_count // DEPTH * tp_count
    step = width // pieces
    slot_count = group * cap
    slot_shape = (DEPTH, pieces, group, cap, step)
    f32, bf16 = jnp.float32, jnp.bfloat16
    dma = pltpu.SemaphoreType.DMA
    vmem = pltpu.VMEM
    hbm = pl.BlockSpec(memory_space=pl.ANY)
    arrays = (*front, *routing)
    return pl.pallas_call(
        functools.partial(layer_kernel, sp_count, tp_count, cap, pieces),
        out_shape=pltpu.VMEM((rows, width), bf16),
        in_specs=[hbm] * (len(arrays) + 4),
        out_specs=pl.BlockSpec(memory_space=pltpu.VMEM),
        scratch_shapes=[vmem(a.shape, a.dtype) for a in arrays]
        + [
            vmem((width, ff), bf16),
            vmem((width, ff), bf16),
            vmem((ff, width), bf16),
            vmem(out_proj.shape, bf16),
            vmem((edge + length, channels), f32),
            vmem((edge + length, lanes), f32),
            vmem((edge, channels + lanes), f32),
            vmem((tp_count, edge, channels + lanes), f32),
            vmem((edge, channels), f32),
            vmem((tp_count, edge, channels), f32),
            vmem((tp_count, rows, channels), bf16),
            vmem((tp_count, rows, channels), bf16),
            vmem((rows, width), f32),
            vmem((DEPTH, 8, rows), f32),
            vmem((DEPTH, slot_count, rows), bf16),
            vmem((slot_count, rows), f32),
            vmem((DEPTH, rows, slot_count), bf16),
            vmem((DEPTH, rows, slot_count), bf16),
            vmem((DEPTH, pieces, rows, step), bf16),
            vmem(slot_shape, bf16),
            vmem(slot_shape, bf16),
            vmem(slot_shape, bf16),
            vmem(slot_shape, bf16),
            vmem((slot_count, ff), bf16),
            vmem((slot_count, 2 * ff), f32),
            vmem((DEPTH - 1, pieces, rows, step), f32),
            vmem((DEPTH, pieces, rows, step), bf16),
            vmem((DEPTH + 1, pieces, rows, step), bf16),
            dma((len(arrays) + 4,)),
            dma((1,)),
            dma((tp_count,)),
            dma((1,)),
            dma((tp_count,)),
            dma((tp_count,)),
            dma((tp_count,)),
            dma((DEPTH + 1,)),
            dma((DEPTH,)),
            dma((3,)),
            dma((DEPTH, pieces)),
            dma((1,)),
            dma((DEPTH, pieces)),
            dma((1,)),
            dma((1,)),
            dma((DEPTH + 1, pieces)),
        ],
        compiler_params=pltpu.CompilerParams(
            collective_id=0, has_side_effects=True, vmem_limit_bytes=56 * 1024 * 1024
        ),
    )(*arrays, gate_proj, up_proj, down_proj, out_proj)


def from_behind(block, axis, distance):
    devices = range(lax.axis_size(axis))
    route = [(i - distance, i) for i in devices if i - distance in devices]
    return lax.ppermute(block, axis, route)


def expert_rows(arrived, gate_weight, up_weight, down_weight):
    gate_value = jnp.dot(arrived, gate_weight, preferred_element_type=jnp.float32)
    up_value = jnp.dot(arrived, up_weight, preferred_element_type=jnp.float32)
    hidden = (jax.nn.silu(gate_value) * up_value).astype(jnp.bfloat16)
    return jnp.dot(hidden, down_weight, preferred_element_type=jnp.float32).astype(jnp.bfloat16)


def on_device(
    conv_input,
    gate_inner,
    gate_outer,
    conv_taps,
    doc_ids,
    residual_in,
    out_proj,
    norm_gain,
    expert_ids,
    expert_weights,
    gate_proj,
    up_proj,
    down_proj,
):
    sp_count, tp_count = lax.axis_size("sp"), lax.axis_size("tp")
    capacity = 2 * residual_in.shape[0] * expert_ids.shape[1] // (sp_count * tp_count)
    if capacity % 16 == 0 and sp_count % DEPTH == 0 and tp_count % 2 == 0:
        docs = doc_ids.reshape(-1, 128)
        front = (conv_input, gate_inner, gate_outer, conv_taps, docs, residual_in, norm_gain[None, :])
        routing = (expert_ids.T, expert_weights.T)
        return run_layer(front, routing, gate_proj, up_proj, down_proj, out_proj, capacity)
    inner_prod = conv_input.astype(jnp.float32) * gate_inner.astype(jnp.float32)
    earlier, earlier_docs = from_behind((inner_prod[-2:], doc_ids[-2:]), "sp", 1)
    padded = jnp.concatenate([earlier, inner_prod], axis=0)
    padded_docs = jnp.concatenate([earlier_docs, doc_ids], axis=0)
    length = inner_prod.shape[0]
    tap_values = conv_taps.astype(jnp.float32)
    one_back = jnp.where(
        (padded_docs[1 : length + 1] == doc_ids)[:, None], padded[1 : length + 1], 0.0
    )
    two_back = jnp.where((padded_docs[:length] == doc_ids)[:, None], padded[:length], 0.0)
    mixed_rows = tap_values[2] * inner_prod + tap_values[1] * one_back + tap_values[0] * two_back
    conv_out = (gate_outer.astype(jnp.float32) * mixed_rows).astype(jnp.bfloat16)
    row_count = residual_in.shape[0]
    regrouped = lax.all_to_all(conv_out, "tp", split_axis=0, concat_axis=1, tiled=True)
    mix = jnp.dot(regrouped, out_proj, preferred_element_type=jnp.float32).astype(jnp.bfloat16)
    carried = residual_in.astype(jnp.float32) + mix.astype(jnp.float32)
    normed = (
        carried * lax.rsqrt(jnp.mean(carried * carried, axis=1, keepdims=True) + 1e-06) * norm_gain
    ).astype(jnp.bfloat16)
    model_width = normed.shape[1]
    choose = expert_ids.shape[1]
    experts_total = sp_count * tp_count
    flat_ids = expert_ids.reshape(-1)
    onehot = (flat_ids[:, None] == jnp.arange(experts_total, dtype=jnp.int32)[None, :]).astype(
        jnp.int32
    )
    slot_rank = jnp.sum((jnp.cumsum(onehot, axis=0) - 1) * onehot, axis=1)
    target = flat_ids * capacity + slot_rank
    sources = jnp.repeat(normed, choose, axis=0)
    outgoing = (
        jnp.zeros((experts_total * capacity, model_width), jnp.bfloat16).at[target].set(sources)
    )
    gate_weight = gate_proj[0]
    up_weight = up_proj[0]
    down_weight = down_proj[0]
    arrived = lax.all_to_all(
        outgoing.reshape(experts_total, capacity, model_width),
        ("sp", "tp"),
        split_axis=0,
        concat_axis=0,
        tiled=True,
    )
    item_count = arrived.shape[1]
    flat_rows = arrived.reshape(-1, model_width)
    result = expert_rows(flat_rows, gate_weight, up_weight, down_weight)
    result = result.reshape(experts_total, item_count, model_width)
    returned = lax.all_to_all(result, ("sp", "tp"), split_axis=0, concat_axis=0, tiled=True)
    picked = (
        returned.reshape(-1, model_width)[target]
        .reshape(row_count, choose, model_width)
        .astype(jnp.float32)
    )
    combined = carried + jnp.sum(expert_weights[:, :, None] * picked, axis=1)
    return combined.astype(jnp.bfloat16)


def solution(mesh):
    in_specs = (
        P("sp", "tp"),
        P("sp", "tp"),
        P("sp", "tp"),
        P(None, "tp"),
        P("sp"),
        P(("sp", "tp"), None),
        P(),
        P(),
        P(("sp", "tp"), None),
        P(("sp", "tp"), None),
        P(("sp", "tp"), None, None),
        P(("sp", "tp"), None, None),
        P(("sp", "tp"), None, None),
    )
    out_specs = P(("sp", "tp"), None)
    return jax.shard_map(
        on_device, mesh=mesh, in_specs=in_specs, out_specs=out_specs, check_vma=False
    )
```
